512 devices in a mesh: ep: 32 (over z, x), tp: 16 (over y, core).
Axes of the slice: x: 4, y: 8, z: 8, core: 2. Of those that a mesh axis runs over, the one named last changes fastest.
Arguments:
- blender_incoming_features: bfloat16 [8192, 4096], P('ep', 'tp'), may hold values from -6 to 6
- entry_latent_matrix: bfloat16 [8192, 2048], P('ep', 'tp'), may hold values from -6 to 6
- exit_latent_matrix: bfloat16 [8192, 2048], P('ep', 'tp'), may hold values from -6 to 6
- unactivated_valve: bfloat16 [8192, 4096], P('ep', 'tp'), may hold values from -6 to 6
- presoftplus_strides: float32 [8192, 64], P('ep', 'tp'), may hold values from -7 to 7
- extra_attenuation: float32 [8192, 64], P('ep', 'tp'), may hold values from -1 to 0
- incoming_feature_kernel: bfloat16 [4, 4096], P(None, 'tp'), may hold values from -3 to 3
- entry_latent_kernel: bfloat16 [4, 2048], P(None, 'tp'), may hold values from -3 to 3
- exit_latent_kernel: bfloat16 [4, 2048], P(None, 'tp'), may hold values from -3 to 3
- stride_offset_vector: float32 [64], P('tp'), may hold values from -1 to 1
- attenuation_speed_exponent: float32 [64], P('tp'), may hold values from -16 to -3
- bypass_coef_vector: float32 [64], P('tp'), may hold values from 0.5 to 4
- cluster_rescale_coefs: bfloat16 [4096], P('tp'), may hold values from 0.099609375 to 1.8984375
- blender_result_matrix: bfloat16 [4096, 2048], P('tp'), may hold values from -0.09375 to 0.09375
- latter_microbatch_activations: bfloat16 [8192, 2048], P('ep'), may hold values from -6 to 6
- specialist_rescale_coefs: bfloat16 [2048], replicated, may hold values from 0.099609375 to 1.8984375
- specialist_valve_matrix: bfloat16 [32, 2048, 4096], P('ep', None, 'tp'), may hold values from -0.125 to 0.125
- specialist_expand_matrix: bfloat16 [32, 2048, 4096], P('ep', None, 'tp'), may hold values from -0.125 to 0.125
- specialist_contract_matrix: bfloat16 [32, 4096, 2048], P('ep', 'tp'), may hold values from -0.125 to 0.125
- specialist_picks: int32 [8192, 2], P('ep'), may hold values from 0 to 31, all different within a row; in each aligned block of 256 rows (0 to 255, 256 to 511, ...) at most 24 rows name the same one
- selected_specialist_coefs: float32 [8192, 2], P('ep'), may hold values from 0.1 to 1
Outputs:
- mixed_a: bfloat16 [8192, 2048], P(('ep', 'tp'))
- mixed_b: bfloat16 [8192, 2048], P('ep', 'tp')
The draws below stay inside these ranges and needn't reach their ends.
Inputs may be any that keep to these rules, and one draw needn't show every extreme that they name: `specialist_picks`: in each aligned block of 256 rows, the rows of one index of ep, no expert is named by more than 24 rows, a bound that some block reaches.
All inputs are finite; a program needn't handle non-finite values.
Results may differ from the reference program's by a relative error of at most 0.019.
Values may be sent and summed in bfloat16 or wider, within the bound.
No kernel may reach another device: no remote copies, remote signals or barrier semaphores. Data moves between devices by JAX's collectives and lax.ppermute only.
A program may use at most 64 MiB of HBM per device.

```python
import math
import jax
import jax.numpy as jnp
import numpy as np
from jax import lax

D = 2048
HEADS = 64
HEAD_DIM = 64
SHARING_CLUSTERS = 16
STATE = 128
CONV = 4
BLOCK = 64
FF = 4096
TOPK = 2
TOK_B_DEV = 256
INNER = 4096
EXPERTS = 32
SEQ_A = 8192
TOKENS_B = 8192
CAP = 24
N_EP = 32
N_TP = 16


def draw_presoftplus_strides(key, part):
    base_key, shift_key = jax.random.split(jax.random.fold_in(key, 3))
    base_draw = jnp.clip(jax.random.normal(base_key, (SEQ_A, HEADS), jnp.float32), -6.0, 6.0)
    offsets = jax.random.uniform(shift_key, (SEQ_A // BLOCK, 1), jnp.float32, -0.8, 0.8)
    return base_draw + jnp.repeat(offsets, BLOCK, axis=0)


def draw_attenuation_speed_exponent(key, part):
    pick_key, slow_key, fast_key = jax.random.split(jax.random.fold_in(key, 7), 3)
    slow_share = 50
    is_slow = jax.random.randint(pick_key, (HEADS,), 0, 100) < slow_share
    slow_rates = jax.random.uniform(slow_key, (HEADS,), jnp.float32, math.log(0.05 / SEQ_A), math.log(0.4 / SEQ_A))
    fast_rates = jax.random.uniform(fast_key, (HEADS,), jnp.float32, math.log(0.01), math.log(0.035))
    return jnp.where(is_slow, slow_rates, fast_rates)


def draw_extra_attenuation(key, part):
    place_key, factor_key = jax.random.split(jax.random.fold_in(key, 13))
    word_locations = jax.random.randint(place_key, (2,), 0, SEQ_A)
    multiplier_entries = jax.random.uniform(factor_key, (HEADS,), jnp.float32, math.log(0.55), math.log(0.8))
    line_ordinal_array = jnp.arange(SEQ_A)
    spike_marker = jnp.any(line_ordinal_array[:, None] == word_locations[None, :], axis=1)
    return jnp.where(spike_marker[:, None], multiplier_entries[None, :], jnp.zeros((), jnp.float32))


def spiked(entries, stream_key, source, target, parts, factor):
    owner, partner = [(jnp.arange(entries.shape[position]) // (entries.shape[position] // parts)).reshape([-1 if axis == position else 1 for axis in range(entries.ndim)]) for position in (source, target)]
    chosen = jax.random.permutation(stream_key, parts)[partner]
    strong = (owner == chosen) | (owner == (partner + parts // 2) % parts)
    return jnp.where(strong, factor * entries, entries)


def shard_levels(own_key, dims, cuts, low, high):
    gain, own = 1.0, jax.random.fold_in(own_key, 6)
    for dim, parts in cuts:
        steps = jnp.exp(jax.random.uniform(jax.random.fold_in(own, dim), (parts,), jnp.float32, low / len(cuts), high / len(cuts)))
        gain = gain * jnp.repeat(steps, dims[dim] // parts).reshape([-1 if axis == dim else 1 for axis in range(len(dims))])
    return gain


def assign_block(stream_key, own, number, rows, number_of, top, limit, skew):
    order = jax.random.permutation(stream_key, number_of)
    crowded, common = portions_of(number_of, rows * top, limit, skew, True), portions_of(number_of, rows * top, limit, skew, False)
    places = jnp.arange(number_of)

    def named(tallies, rotation):
        used = int((tallies > 0).sum())
        fixed = max(1, used // 4)
        moved = fixed + (places - fixed + rotation * (used - fixed)) % max(1, number_of - fixed)
        return jnp.zeros((number_of,), jnp.int32).at[order[jnp.where(places < fixed, places, moved)]].set(jnp.asarray(tallies, jnp.int32))

    tallies = jnp.where(number % 4 == 0, named(crowded, number // 4), named(common, number - number // 4 - 1))
    mixed = jax.random.permutation(jax.random.fold_in(own, 3), number_of)
    giver, receiver = mixed[0:number_of // 2 * 2:2], mixed[1:number_of // 2 * 2:2]
    margin = jnp.minimum(tallies[giver] - 1, limit - tallies[receiver]) // 2
    margin = jnp.where((giver == order[0]) | (receiver == order[0]) | (tallies[receiver] == 0), 0, jnp.maximum(margin, 0))
    moved = jax.random.randint(jax.random.fold_in(own, 4), (number_of // 2,), 0, 1 << 20) % (margin + 1)
    tallies = tallies.at[giver].add(-moved).at[receiver].add(moved)
    items = jnp.searchsorted(jnp.cumsum(tallies), jnp.arange(rows * top), side="right").astype(jnp.int32)
    grid = items.reshape(top, rows).T
    grid = grid[jax.random.permutation(jax.random.fold_in(own, 1), rows)]
    rotation = jax.random.randint(jax.random.fold_in(own, 2), (rows, 1), 0, top)
    return jnp.take_along_axis(grid, (jnp.arange(top)[None, :] + rotation) % top, axis=1)


def portions_of(count, total, reach, skew, full):
    portions = [(1 << 20) // math.isqrt(standing ** skew) + 1 for standing in range(1, count + 1)]
    largest = reach if full else min(reach, max(-(-total // count), total * portions[0] // sum(portions)))
    least = 1 if total - largest >= count - 1 else 0
    given, surplus = [largest] + [least] * (count - 1), total - largest - least * (count - 1)
    while surplus > 0:
        movable = [i for i in range(1, count) if given[i] < largest] or [i for i in range(1, count) if given[i] < reach]
        pool, remaining = sum([portions[i] for i in movable]), surplus
        for i in movable:
            extra = min(reach - given[i], max(1, remaining * portions[i] // pool), surplus)
            given[i] = given[i] + extra
            surplus = surplus - extra
    return np.array(given)


def scatter_about(own_key, shape, width, bound, shards=(), held_as=jnp.bfloat16):
    result = jax.random.normal(own_key, shape, jnp.float32) * width
    if len(shards) > 0:
        result = shard_levels(own_key, shape, shards, -0.22, 0.18) * result
    return jnp.clip(result, min=-bound, max=bound).astype(held_as)


def noise_with(key, extent, deviation, limit, cuts, heavy, kind=jnp.bfloat16):
    entries = deviation * jax.random.normal(key, extent, jnp.float32)
    if cuts:
        entries = entries * shard_levels(key, extent, cuts, -0.22, 0.18)
    return jnp.clip(spiked(entries, jax.random.fold_in(key, 3), *heavy), -limit, limit).astype(kind)


def setup_inputs(seed: int = 0) -> dict:
    streams_of = jax.random.split(jax.random.key(seed), 22)
    blender_incoming_features = scatter_about(streams_of[0], (SEQ_A, INNER), 1.0, 6.0, ((0, 32), (1, 16)))
    entry_latent_matrix = scatter_about(streams_of[1], (SEQ_A, SHARING_CLUSTERS * STATE), 1.0, 6.0, ((0, 32), (1, 16)))
    exit_latent_matrix = scatter_about(streams_of[2], (SEQ_A, SHARING_CLUSTERS * STATE), 1.0, 6.0, ((0, 32), (1, 16)))
    unactivated_valve = scatter_about(streams_of[3], (SEQ_A, INNER), 1.0, 6.0, ((0, 32), (1, 16)))
    presoftplus_strides = draw_presoftplus_strides(jax.random.fold_in(streams_of[21], 71), 0)
    extra_attenuation = draw_extra_attenuation(jax.random.fold_in(streams_of[21], 71), 0)
    incoming_feature_kernel = scatter_about(streams_of[6], (CONV, INNER), CONV ** -0.5, 3.0, ((1, 16),))
    entry_latent_kernel = scatter_about(streams_of[7], (CONV, SHARING_CLUSTERS * STATE), CONV ** -0.5, 3.0, ((1, 16),))
    exit_latent_kernel = scatter_about(streams_of[8], (CONV, SHARING_CLUSTERS * STATE), CONV ** -0.5, 3.0, ((1, 16),))
    stride_offset_vector = jnp.clip(jax.random.uniform(streams_of[9], (HEADS,), jnp.float32, -1.0, 1.0) * shard_levels(streams_of[9], (HEADS,), ((0, 16),), -0.4, 0.0), -1.0, 1.0)
    attenuation_speed_exponent = draw_attenuation_speed_exponent(jax.random.fold_in(streams_of[21], 71), 0)
    bypass_coef_vector = jnp.clip(jnp.exp(math.log(4.0) - 2.0794415 * jax.random.uniform(streams_of[11], (HEADS,), jnp.float32) ** shard_levels(streams_of[11], (HEADS,), ((0, 16),), -0.2, 0.2)), 0.5, 4.0)
    cluster_rescale_coefs = jnp.clip(1.0 + 0.18 * jax.random.normal(streams_of[12], (INNER,), jnp.float32), 0.099609375, 1.8984375).astype(jnp.bfloat16)
    blender_result_matrix = scatter_about(streams_of[13], (INNER, D), INNER ** -0.5, 0.09375, ((0, 16),))
    latter_microbatch_activations = scatter_about(streams_of[14], (TOKENS_B, D), 1.0, 6.0, ((0, 32),))
    specialist_rescale_coefs = jnp.clip(1.0 + 0.18 * jax.random.normal(streams_of[15], (D,), jnp.float32), 0.099609375, 1.8984375).astype(jnp.bfloat16)
    specialist_valve_matrix = scatter_about(streams_of[16], (EXPERTS, D, FF), D ** -0.5, 0.125, ((0, 32), (2, 16)))
    specialist_expand_matrix = scatter_about(streams_of[17], (EXPERTS, D, FF), D ** -0.5, 0.125, ((0, 32), (2, 16)))
    specialist_contract_matrix = noise_with(streams_of[18], (EXPERTS, FF, D), FF ** -0.5, 0.125, ((0, 32), (1, 16)), (1, 2, 16, 2.0))
    specialist_picks_keys = jax.random.split(jax.random.fold_in(streams_of[19], 1), TOKENS_B // TOK_B_DEV)
    specialist_picks_turns = jax.random.permutation(jax.random.fold_in(streams_of[19], 3), TOKENS_B // TOK_B_DEV)
    specialist_picks = jax.vmap(lambda own, number: assign_block(jax.random.fold_in(streams_of[19], 2), own, number, TOK_B_DEV, EXPERTS, TOPK, CAP, 2))(specialist_picks_keys, specialist_picks_turns).reshape((TOKENS_B, TOPK))
    selected_specialist_coefs = jnp.clip(0.1 + 0.9 * jax.random.uniform(streams_of[20], (TOKENS_B, TOPK), jnp.float32) ** shard_levels(streams_of[20], (TOKENS_B, TOPK), ((0, 32),), -0.2, 0.2), 0.1, 1.0)
    return {"blender_incoming_features": blender_incoming_features, "entry_latent_matrix": entry_latent_matrix, "exit_latent_matrix": exit_latent_matrix, "unactivated_valve": unactivated_valve, "presoftplus_strides": presoftplus_strides, "extra_attenuation": extra_attenuation, "incoming_feature_kernel": incoming_feature_kernel, "entry_latent_kernel": entry_latent_kernel, "exit_latent_kernel": exit_latent_kernel, "stride_offset_vector": stride_offset_vector, "attenuation_speed_exponent": attenuation_speed_exponent, "bypass_coef_vector": bypass_coef_vector, "cluster_rescale_coefs": cluster_rescale_coefs, "blender_result_matrix": blender_result_matrix, "latter_microbatch_activations": latter_microbatch_activations, "specialist_rescale_coefs": specialist_rescale_coefs, "specialist_valve_matrix": specialist_valve_matrix, "specialist_expand_matrix": specialist_expand_matrix, "specialist_contract_matrix": specialist_contract_matrix, "specialist_picks": specialist_picks, "selected_specialist_coefs": selected_specialist_coefs}


NORM_EPS = 1e-06
HIGHEST = lax.Precision.HIGHEST

def conv_silu(inputs, weight):
    tap_count = weight.shape[0]
    context_span = inputs.shape[0]
    padded = jnp.pad(inputs.astype(jnp.float32), ((tap_count - 1, 0), (0, 0)))
    kernel = weight.astype(jnp.float32)
    running_total = kernel[0] * padded[0:context_span]
    for offset in range(1, tap_count):
        running_total = running_total + kernel[offset] * padded[offset:offset + context_span]
    return jax.nn.silu(running_total)

def block_step(carry_state, inputs):
    scaled_x, b_block, c_block, log_block = inputs
    context_span = log_block.shape[0]
    running = jnp.cumsum(log_block, axis=0)
    causal = (jnp.arange(context_span)[:, None] >= jnp.arange(context_span)[None, :])[:, :, None, None]
    log_gap = running[:, None] - running[None, :]
    weights = jnp.where(causal, jnp.exp(jnp.where(causal, log_gap, 0.0)), 0.0)
    scores = jnp.einsum('lgn,sgn->lsg', c_block, b_block, preferred_element_type=jnp.float32)
    inside = jnp.einsum('lsgj,sgjp->lgjp', scores[..., None] * weights, scaled_x, precision=HIGHEST)
    c_wide = c_block.astype(jnp.float32)
    b_wide = b_block.astype(jnp.float32)
    before = jnp.einsum('lgn,gjpn->lgjp', c_wide, carry_state, precision=HIGHEST) * jnp.exp(running)[..., None]
    to_end = jnp.exp(running[-1] - running)
    carry_state = carry_state * jnp.exp(running[-1])[..., None, None] + jnp.einsum('sgn,sgjp->gjpn', b_wide, scaled_x * to_end[..., None], precision=HIGHEST)
    return (carry_state, inside + before)

def rounded_pieces(left, right, pieces):
    block_width = left.shape[1] // pieces
    running_total = jnp.zeros((left.shape[0], right.shape[1]), jnp.float32)
    for piece_index in range(pieces):
        block_term = jnp.dot(left[:, piece_index * block_width:(piece_index + 1) * block_width], right[piece_index * block_width:(piece_index + 1) * block_width], preferred_element_type=jnp.float32).astype(jnp.bfloat16)
        running_total = running_total + lax.optimization_barrier(block_term).astype(jnp.float32)
    return running_total.astype(jnp.bfloat16)

def reference(blender_incoming_features, entry_latent_matrix, exit_latent_matrix, unactivated_valve, presoftplus_strides, extra_attenuation, incoming_feature_kernel, entry_latent_kernel, exit_latent_kernel, stride_offset_vector, attenuation_speed_exponent, bypass_coef_vector, cluster_rescale_coefs, blender_result_matrix, latter_microbatch_activations, specialist_rescale_coefs, specialist_valve_matrix, specialist_expand_matrix, specialist_contract_matrix, specialist_picks, selected_specialist_coefs):
    context_span = blender_incoming_features.shape[0]
    members_within_cluster = HEADS // SHARING_CLUSTERS
    conv_x_out = conv_silu(blender_incoming_features, incoming_feature_kernel).reshape(context_span, SHARING_CLUSTERS, members_within_cluster, HEAD_DIM)
    conv_b_out = conv_silu(entry_latent_matrix, entry_latent_kernel).astype(jnp.bfloat16).reshape(context_span, SHARING_CLUSTERS, STATE)
    conv_c_out = conv_silu(exit_latent_matrix, exit_latent_kernel).astype(jnp.bfloat16).reshape(context_span, SHARING_CLUSTERS, STATE)
    stride_amount = jax.nn.softplus(presoftplus_strides + stride_offset_vector[None, :])
    attenuation_exponent = (-jnp.exp(attenuation_speed_exponent)[None, :] * stride_amount + extra_attenuation).reshape(context_span, SHARING_CLUSTERS, members_within_cluster)
    scaled_x = conv_x_out * stride_amount.reshape(context_span, SHARING_CLUSTERS, members_within_cluster)[..., None]
    blocks = context_span // BLOCK

    def as_blocks(array_value):
        return array_value.reshape((blocks, BLOCK) + array_value.shape[1:])
    start_state = jnp.zeros((SHARING_CLUSTERS, members_within_cluster, HEAD_DIM, STATE), jnp.float32)
    _, block_out = lax.scan(block_step, start_state, (as_blocks(scaled_x), as_blocks(conv_b_out), as_blocks(conv_c_out), as_blocks(attenuation_exponent)))
    ssd_out = block_out.reshape(context_span, SHARING_CLUSTERS, members_within_cluster, HEAD_DIM) + bypass_coef_vector.reshape(SHARING_CLUSTERS, members_within_cluster)[None, :, :, None] * conv_x_out
    gated_out = ssd_out.reshape(context_span, INNER) * jax.nn.silu(unactivated_valve.astype(jnp.float32))
    grouped = gated_out.reshape(context_span, SHARING_CLUSTERS, INNER // SHARING_CLUSTERS)
    grouped = grouped * lax.rsqrt(lax.optimization_barrier(jnp.mean(grouped * grouped, axis=-1, keepdims=True)) + NORM_EPS)
    normed = (grouped.reshape(context_span, INNER) * cluster_rescale_coefs.astype(jnp.float32)).astype(jnp.bfloat16)
    mixed_a = rounded_pieces(normed, blender_result_matrix, N_TP)
    widened = latter_microbatch_activations.astype(jnp.float32)
    normed_b = (widened * lax.rsqrt(lax.optimization_barrier(jnp.mean(widened * widened, axis=-1, keepdims=True)) + NORM_EPS) * specialist_rescale_coefs.astype(jnp.float32)).astype(jnp.bfloat16)
    flat_routes = specialist_picks.reshape(-1).astype(jnp.int32)
    assigned = flat_routes.shape[0]
    sorted_order = jnp.argsort(flat_routes, stable=True).astype(jnp.int32)
    routes_sorted = flat_routes[sorted_order]
    tokens_sorted = (sorted_order // TOPK).astype(jnp.int32)
    counts = lax.optimization_barrier(jnp.sum((flat_routes[:, None] == jnp.arange(EXPERTS, dtype=jnp.int32)[None, :]).astype(jnp.int32), axis=0)).astype(jnp.int32)
    starts = (jnp.cumsum(counts) - counts).astype(jnp.int32)
    place_sorted = (jnp.arange(assigned, dtype=jnp.int32) - starts[routes_sorted]).astype(jnp.int32)
    places = jnp.zeros((assigned,), jnp.int32).at[sorted_order].set(place_sorted)
    capacity_all = N_EP * CAP

    def one_expert(expert):
        slots = jnp.arange(capacity_all, dtype=jnp.int32)
        is_valid = slots < counts[expert]
        token_ids = tokens_sorted[jnp.minimum(starts[expert] + slots, assigned - 1)]
        chosen = jnp.where(is_valid[:, None], normed_b[token_ids], jnp.zeros((), jnp.bfloat16))
        gate_sum = jnp.dot(chosen, specialist_valve_matrix[expert], preferred_element_type=jnp.float32)
        up_sum = jnp.dot(chosen, specialist_expand_matrix[expert], preferred_element_type=jnp.float32)
        hidden = (jax.nn.silu(gate_sum) * up_sum).astype(jnp.bfloat16)
        return rounded_pieces(hidden, specialist_contract_matrix[expert], N_TP)
    results = lax.map(one_expert, jnp.arange(EXPERTS, dtype=jnp.int32))
    picked = results[flat_routes, places].astype(jnp.float32) * selected_specialist_coefs.reshape(assigned, 1)
    mixed_b = lax.optimization_barrier(jnp.sum(picked.reshape(assigned // TOPK, TOPK, D), axis=1)).astype(jnp.bfloat16)
    return (mixed_a, mixed_b)
```

```python
import jax
import jax.numpy as jnp
from jax import lax
from jax.experimental import pallas as pl
from jax.experimental.pallas import tpu as pltpu
from jax.sharding import Mesh
from jax.sharding import PartitionSpec as P

HEADS = 64
HEAD_DIM = 64
SHARING_CLUSTERS = 16
STATE = 128
TOPK = 2
EP = ("ep_0", "ep_1")
TP = ("tp_0", "tp_1")
EP_TP = ("ep_0", "ep_1", "tp_0", "tp_1")
RIM = 8
PIECE = 8

NORM_EPS = 1e-06
F32 = jnp.float32
BF16 = jnp.bfloat16
VMEM = pl.BlockSpec(memory_space=pltpu.VMEM)
SMEM = pl.BlockSpec(memory_space=pltpu.SMEM)


def call(body, outs, ins, flops, scratch=(), smem=0):
    return pl.pallas_call(
        body,
        out_shape=outs,
        in_specs=[SMEM] * smem + [VMEM] * (len(ins) - smem),
        out_specs=jax.tree.map(lambda _: VMEM, outs),
        scratch_shapes=scratch,
        cost_estimate=pl.CostEstimate(flops=flops, bytes_accessed=1 << 20, transcendentals=0),
    )(*ins)


def shaped(*shape, dtype=BF16):
    return jax.ShapeDtypeStruct(shape, dtype)


def iota(shape, dim):
    return lax.broadcasted_iota(jnp.int32, shape, dim)


def silu(v):
    return v * jax.nn.sigmoid(v)


def dot(a, b, contract=(1, 0)):
    return lax.dot_general(
        a, b, (((contract[0],), (contract[1],)), ((), ())), preferred_element_type=F32
    )


def spread(columns, width):
    lane_head = iota((columns.shape[0], 4 * width), 1) // width
    wide = columns[:, 0:1]
    for head in range(1, 4):
        wide = jnp.where(lane_head == head, columns[:, head : head + 1], wide)
    return wide


def front_body(
    place,
    tokens,
    token_gain,
    picks,
    x_in,
    b_in,
    c_in,
    rim,
    x_taps,
    b_taps,
    c_taps,
    strides,
    extra,
    offset,
    speed,
    send,
    x_out,
    b_out,
    c_out,
    columns_out,
    rows_out,
    slots_out,
    joined,
):
    count, width = x_in.shape
    state = b_in.shape[1]
    experts, rows, lanes = send.shape
    capacity = rows - 2 * PIECE

    joined[0:RIM, :] = rim[...].astype(F32)
    joined[RIM:, 0:width] = x_in[...].astype(F32)
    joined[RIM:, width : width + state] = b_in[...].astype(F32)
    joined[RIM:, width + state :] = c_in[...].astype(F32)

    def filtered(first, size, taps_ref):
        taps = taps_ref[...].astype(F32)
        total = None
        for j in range(taps.shape[0]):
            start = RIM - taps.shape[0] + 1 + j
            term = taps[j : j + 1] * joined[start : start + count, first : first + size]
            total = term if total is None else total + term
        return silu(total)

    x = filtered(0, width, x_taps)
    b = filtered(width, state, b_taps).astype(BF16)
    c = filtered(width + state, state, c_taps).astype(BF16)
    x_out[...] = x
    b_out[...] = b
    c_out[...] = c

    raw = strides[...] + offset[...]
    step = jnp.maximum(raw, 0.0) + jnp.log1p(jnp.exp(-jnp.abs(raw)))
    total = -jnp.exp(speed[...]) * step + extra[...]
    both = jnp.concatenate([total, step], axis=0)
    lane = iota(both.shape, 1)
    shift = 1
    while shift < count:
        moved = jnp.where((lane >= shift), pltpu.roll(both, shift, axis=1), 0.0)
        both = jnp.where(iota(both.shape, 0) < 4, both + moved, both)
        shift *= 2
    columns = both.T
    rows_out[...] = both
    columns_out[...] = columns
    running, step_column = columns[:, 0:4], columns[:, 4:8]
    last = columns[count - 1 : count, 0:4]
    weight = step_column * jnp.exp(last - running)
    weighted = (x * spread(weight, HEAD_DIM)).astype(BF16)
    end_state = dot(weighted, b, (0, 0)).astype(BF16)
    high = last.astype(BF16).astype(F32)
    low = last - high
    half = iota((PIECE, lanes), 1) < lanes // 2

    data = tokens[...].astype(F32)
    scale = lax.rsqrt(jnp.mean(data * data, axis=1, keepdims=True) + NORM_EPS)
    first = pl.multiple_of(place[0] * lanes, lanes)
    chosen = tokens[:, pl.ds(first, lanes)].astype(F32)
    gain = token_gain[:, pl.ds(first, lanes)].astype(F32)
    chosen = (chosen * scale * gain).astype(BF16)
    token_count = tokens.shape[0]
    expert = iota((experts, token_count), 0)
    earlier = (
        iota((token_count, token_count), 0) < iota((token_count, token_count), 1)
    ).astype(BF16)
    base = jnp.zeros((experts, 1), F32)
    slot_ids = iota((experts * capacity, token_count), 0)
    placing = None
    for k in range(TOPK):
        pick = picks[k : k + 1, :]
        named = (expert == pick).astype(F32)
        rank = base + dot(named.astype(BF16), earlier)
        rank = jnp.sum(named * rank, axis=0, keepdims=True)
        slot = pick * capacity + rank.astype(jnp.int32)
        slots_out[k : k + 1, :] = slot
        base = base + jnp.sum(named, axis=1, keepdims=True)
        hit = slot_ids == slot
        placing = hit if placing is None else placing | hit
    routed = dot(placing.astype(F32).astype(BF16), chosen).astype(BF16)
    for e in range(experts):
        head = e * PIECE // HEAD_DIM
        send[e, 0:capacity, :] = routed[e * capacity : (e + 1) * capacity]
        send[e, capacity : capacity + PIECE, :] = end_state[e * PIECE : (e + 1) * PIECE]
        send[e, capacity + PIECE :, :] = jnp.where(
            half, high[:, head : head + 1], low[:, head : head + 1]
        ).astype(BF16)


def enter_body(got, enter, tokens):
    sources, rows, lanes = got.shape
    capacity = rows - 2 * PIECE
    tokens[...] = got[:, 0:capacity, :].reshape(sources * capacity, lanes)
    size = sources * PIECE
    piece = got[:, capacity : capacity + PIECE, :].reshape(size, lanes)
    logs = got[:, capacity + PIECE :, :].reshape(size, lanes).astype(F32)
    logs = logs[:, 0:1] + logs[:, lanes // 2 : lanes // 2 + 1]
    row, column = iota((size, size), 0), iota((size, size), 1)
    before = column // PIECE < row // PIECE
    mean = jnp.where(before, 1.0 / PIECE, 0.0).astype(BF16)
    wide = jnp.broadcast_to(logs, (size, lanes))
    high = wide.astype(BF16)
    mid = (wide - high.astype(F32)).astype(BF16)
    low = (wide - high.astype(F32) - mid.astype(F32)).astype(BF16)
    earlier = dot(mean, high) + dot(mean, mid) + dot(mean, low)
    through = (earlier + wide).T[0:1, :]
    keep = before & (column % PIECE == row % PIECE)
    gap = jnp.where(keep, earlier[:, 0:1] - through, 0.0)
    decay = jnp.where(keep, jnp.exp(gap), 0.0)
    decay_high = decay.astype(BF16)
    decay_low = (decay - decay_high.astype(F32)).astype(BF16)
    result = dot(decay_high, piece) + dot(decay_low, piece)
    enter[...] = result.astype(BF16).reshape(sources, PIECE, lanes)


def inside_body(x_ref, b_ref, c_ref, columns, rows, bypass, out):
    count = x_ref.shape[0]
    scores = dot(c_ref[...], b_ref[...], (1, 1))
    causal = iota((count, count), 0) >= iota((count, count), 1)
    for head in range(4):
        part = slice(head * HEAD_DIM, (head + 1) * HEAD_DIM)
        gap = columns[:, head : head + 1] - rows[head : head + 1, :]
        weights = jnp.where(causal, jnp.exp(jnp.where(causal, gap, 0.0)), 0.0)
        x = x_ref[:, part]
        scaled = (x * columns[:, 4 + head : 5 + head]).astype(BF16)
        inside = dot((scores * weights).astype(BF16), scaled)
        out[:, part] = inside + bypass[head] * x


def finish_body(place, y, c, columns, enter, valve, gain, result, mine, other, normed):
    carried = dot(c[...], enter[...], (1, 1))
    carried = carried * spread(jnp.exp(columns[:, 0:4]), HEAD_DIM)
    gated = (y[...] + carried) * silu(valve[...].astype(F32))
    scale = lax.rsqrt(jnp.mean(gated * gated, axis=1, keepdims=True) + NORM_EPS)
    normed[...] = gated * scale * gain[...].astype(F32)
    chips, rows, width = mine.shape
    for target, core in ((mine, place[0]), (other, 1 - place[0])):
        parts = [
            normed[pl.ds(pl.multiple_of(2 * rows * k + rows * core, 8), rows), :]
            for k in range(chips)
        ]
        left = jnp.concatenate(parts, axis=0).astype(BF16)
        block = 512
        for first in range(0, width, block):
            product = dot(left, result[:, first : first + block]).astype(BF16)
            target[:, :, first : first + block] = product.reshape(chips, rows, block)


def expert_body(place, own, far, valve, expand, contract, mine, other):
    chips, total, lanes = own.shape
    core = place[0]
    half = chips * lanes
    hidden_width = valve.shape[1]
    block = 256
    near_rows = pl.ds(pl.multiple_of(core * half, half), half)
    far_rows = pl.ds(pl.multiple_of((1 - core) * half, half), half)

    def columns_of(which):
        return jnp.concatenate(
            [
                contract[:, pl.ds(pl.multiple_of((2 * k + which) * lanes, lanes), lanes)]
                for k in range(chips)
            ],
            axis=1,
        )

    def step(i, _):
        at = pl.ds(pl.multiple_of(i * block, block), block)
        near_x = jnp.concatenate([own[k, at, :] for k in range(chips)], axis=1)
        far_x = jnp.concatenate([far[k, at, :] for k in range(chips)], axis=1)
        gate = dot(near_x, valve[near_rows, :]) + dot(far_x, valve[far_rows, :])
        up = dot(near_x, expand[near_rows, :]) + dot(far_x, expand[far_rows, :])
        hidden = (silu(gate) * up).astype(BF16)
        for target, which in ((mine, core), (other, 1 - core)):
            product = dot(hidden, columns_of(which)).astype(BF16)
            for k in range(chips):
                target[k, at, :] = product[:, k * lanes : (k + 1) * lanes]
        return 0

    lax.fori_loop(0, total // block, step, 0)


def combine_body(got, slots, coefs, out):
    sources, capacity, lanes = got.shape
    rows = got[...].reshape(sources * capacity, lanes)
    slot_ids = iota((rows.shape[0], slots.shape[1]), 0)
    padded = jnp.concatenate([coefs[...]] * (8 // TOPK), axis=0)
    columns = padded.T
    total = None
    for k in range(TOPK):
        chosen = (slot_ids == slots[k : k + 1, :]).astype(F32).astype(BF16)
        term = dot(chosen, rows, (0, 0)) * columns[:, k : k + 1]
        total = term if total is None else total + term
    out[...] = total.astype(BF16)


def local(
    blender_incoming_features,
    entry_latent_matrix,
    exit_latent_matrix,
    unactivated_valve,
    presoftplus_strides,
    extra_attenuation,
    incoming_feature_kernel,
    entry_latent_kernel,
    exit_latent_kernel,
    stride_offset_vector,
    attenuation_speed_exponent,
    bypass_coef_vector,
    cluster_rescale_coefs,
    blender_result_matrix,
    latter_microbatch_activations,
    specialist_rescale_coefs,
    specialist_valve_matrix,
    specialist_expand_matrix,
    specialist_contract_matrix,
    specialist_picks,
    selected_specialist_coefs,
):
    ep_count, chips = lax.axis_size(EP), lax.axis_size("tp_0")
    chip, core = lax.axis_index("tp_0"), lax.axis_index("tp_1")
    count, width = blender_incoming_features.shape
    state = entry_latent_matrix.shape[1]
    token_count, model_width = latter_microbatch_activations.shape
    capacity = 3 * token_count * TOPK // (2 * ep_count)
    lanes = model_width // lax.axis_size(TP)
    total_rows = ep_count * capacity
    swap = [(0, 1), (1, 0)]
    core_at = core.reshape(1)

    rim = jnp.concatenate(
        [
            blender_incoming_features[count - RIM :],
            entry_latent_matrix[count - RIM :],
            exit_latent_matrix[count - RIM :],
        ],
        axis=1,
    )
    rim = lax.ppermute(rim, EP, [(i, i + 1) for i in range(ep_count - 1)])

    send, x, b, c, columns, rows, slots = call(
        front_body,
        (
            shaped(ep_count, capacity + 2 * PIECE, lanes),
            shaped(count, width, dtype=F32),
            shaped(count, state),
            shaped(count, state),
            shaped(count, 8, dtype=F32),
            shaped(8, count, dtype=F32),
            shaped(TOPK, token_count, dtype=jnp.int32),
        ),
        (
            (core * chips + chip).reshape(1),
            latter_microbatch_activations,
            specialist_rescale_coefs.reshape(1, -1),
            specialist_picks.T,
            blender_incoming_features,
            entry_latent_matrix,
            exit_latent_matrix,
            rim,
            incoming_feature_kernel,
            entry_latent_kernel,
            exit_latent_kernel,
            presoftplus_strides.T,
            extra_attenuation.T,
            stride_offset_vector.reshape(-1, 1),
            attenuation_speed_exponent.reshape(-1, 1),
        ),
        1 << 30,
        scratch=(pltpu.VMEM((RIM + count, width + 2 * state), F32),),
        smem=1,
    )
    got = lax.all_to_all(send, EP, 0, 0, tiled=True)
    enter, tokens = call(
        enter_body,
        (shaped(ep_count, PIECE, lanes), shaped(total_rows, lanes)),
        (got,),
        1 << 28,
    )
    own = lax.all_to_all(
        jnp.broadcast_to(tokens, (chips, total_rows, lanes)), "tp_0", 0, 0, tiled=True
    )
    enter = lax.all_to_all(enter, EP, 0, 0, tiled=True).reshape(width, state)
    y = inside(bypass_coef_vector, x, b, c, columns, rows)
    mine_a, other_a = call(
        finish_body,
        (shaped(chips, count // (2 * chips), model_width),) * 2,
        (
            core_at,
            y,
            c,
            columns,
            enter,
            unactivated_valve,
            cluster_rescale_coefs.reshape(1, -1),
            blender_result_matrix,
        ),
        1 << 31,
        scratch=(pltpu.VMEM((count, width), F32),),
        smem=1,
    )
    other_a = lax.ppermute(other_a, "tp_1", swap)
    parts_a = (mine_a.astype(F32) + other_a.astype(F32)).astype(BF16)
    parts_a = lax.all_to_all(parts_a, "tp_0", 0, 0, tiled=True)
    mixed_a = jnp.sum(parts_a.astype(F32), axis=0).astype(BF16)

    far = lax.ppermute(own, "tp_1", swap)
    mine, other = call(
        expert_body,
        (shaped(chips, total_rows, lanes),) * 2,
        (
            core_at,
            own,
            far,
            specialist_valve_matrix.reshape(model_width, -1),
            specialist_expand_matrix.reshape(model_width, -1),
            specialist_contract_matrix.reshape(-1, model_width),
        ),
        1 << 32,
        smem=1,
    )
    other = lax.ppermute(other, "tp_1", swap)
    parts = (mine.astype(F32) + other.astype(F32)).astype(BF16)
    parts = lax.all_to_all(parts, "tp_0", 0, 0, tiled=True)
    summed = jnp.sum(parts.astype(F32), axis=0).astype(BF16)
    returned = lax.all_to_all(
        summed.reshape(ep_count, capacity, lanes), EP, 0, 0, tiled=True
    )
    mixed_b = call(
        combine_body,
        shaped(token_count, lanes),
        (returned, slots, selected_specialist_coefs.T),
        1 << 28,
    )
    return (mixed_a, mixed_b)


def inside(bypass, x, b, c, columns, rows):
    def body(bypass, x, b, c, columns, rows, out):
        inside_body(x, b, c, columns, rows, bypass, out)

    return call(
        body,
        shaped(*x.shape, dtype=F32),
        (bypass, x, b, c, columns, rows),
        1 << 31,
        smem=1,
    )


def solution(mesh):
    split = Mesh(mesh.devices.reshape(8, 4, 8, 2), ("ep_0", "ep_1", "tp_0", "tp_1"))
    in_specs = (
        P(EP, TP),
        P(EP, TP),
        P(EP, TP),
        P(EP, TP),
        P(EP, TP),
        P(EP, TP),
        P(None, TP),
        P(None, TP),
        P(None, TP),
        P(TP),
        P(TP),
        P(TP),
        P(TP),
        P(TP, None),
        P(EP, None),
        P(),
        P(EP, None, TP),
        P(EP, None, TP),
        P(EP, TP, None),
        P(EP, None),
        P(EP, None),
    )
    out_specs = (P(EP_TP, None), P(EP, TP))
    return jax.shard_map(local, mesh=split, in_specs=in_specs, out_specs=out_specs, check_vma=False)
```

```python
import functools

import jax
import jax.numpy as jnp
from jax import lax
from jax.experimental import pallas as pl
from jax.experimental.pallas import tpu as pltpu
from jax.sharding import Mesh
from jax.sharding import PartitionSpec as P


HEAD_DIM = 64
TOPK = 2
EP = ("ep_0", "ep_1")
TP = ("tp_0", "tp_1")
EP_TP = ("ep_0", "ep_1", "tp_0", "tp_1")
RIM = 8
PIECE = 8

NORM_EPS = 1e-06
F32 = jnp.float32
BF16 = jnp.bfloat16
VMEM = pl.BlockSpec(memory_space=pltpu.VMEM)
SMEM = pl.BlockSpec(memory_space=pltpu.SMEM)


def call(body, outs, ins, flops, room, scratch=(), smem=0):
    return pl.pallas_call(
        body,
        out_shape=outs,
        in_specs=[SMEM] * smem + [VMEM] * (len(ins) - smem),
        out_specs=jax.tree.map(lambda _: VMEM, outs),
        scratch_shapes=scratch,
        cost_estimate=pl.CostEstimate(flops=flops, bytes_accessed=1 << 20, transcendentals=0),
        compiler_params=pltpu.CompilerParams(vmem_limit_bytes=room << 20),
    )(*ins)


def shaped(*shape, dtype=BF16):
    return jax.ShapeDtypeStruct(shape, dtype)


def iota(shape, dim):
    return lax.broadcasted_iota(jnp.int32, shape, dim)


def silu(v):
    return v * jax.nn.sigmoid(v)


def dot(a, b, contract=(1, 0)):
    return lax.dot_general(
        a, b, (((contract[0],), (contract[1],)), ((), ())), preferred_element_type=F32
    )


def spread(columns, width):
    lane_head = iota((columns.shape[0], 4 * width), 1) // width
    wide = columns[:, 0:1]
    for head in range(1, 4):
        wide = jnp.where(lane_head == head, columns[:, head : head + 1], wide)
    return wide


def route_body(experts, place, tokens, token_gain, picks, routed, slots_out):
    lanes = token_gain.shape[1]
    total_rows, token_count = routed.shape[0], tokens.shape[0]
    capacity = total_rows // experts
    data = tokens[...].astype(F32)
    scale = lax.rsqrt(jnp.mean(data * data, axis=1, keepdims=True) + NORM_EPS)
    first = pl.multiple_of(place[0] * lanes, lanes)
    chosen = tokens[:, pl.ds(first, 2 * lanes)].astype(F32)
    gain = jnp.concatenate([token_gain[pl.ds(place[0] + k, 1), :] for k in range(2)], axis=1)
    chosen = (chosen * scale * gain).astype(BF16)
    expert = iota((experts, token_count), 0)
    earlier = (
        iota((token_count, token_count), 0) < iota((token_count, token_count), 1)
    ).astype(BF16)
    base = jnp.zeros((experts, 1), F32)
    slot_ids = iota((total_rows, token_count), 0)
    placing = None
    for k in range(TOPK):
        pick = picks[k : k + 1, :]
        named = (expert == pick).astype(F32)
        rank = base + dot(named.astype(BF16), earlier)
        rank = jnp.sum(named * rank, axis=0, keepdims=True)
        slot = pick * capacity + rank.astype(jnp.int32)
        slots_out[k : k + 1, :] = slot
        base = base + jnp.sum(named, axis=1, keepdims=True)
        hit = slot_ids == slot
        placing = hit if placing is None else placing | hit
    routed[...] = dot(placing.astype(F32).astype(BF16), chosen).astype(BF16)


def filter_body(
    offset,
    speed,
    routed,
    x_in,
    b_in,
    c_in,
    rim,
    x_taps,
    b_taps,
    c_taps,
    strides,
    extra,
    send,
    x_out,
    b_out,
    c_out,
    columns_out,
    rows_out,
    joined,
):
    count, width = x_in.shape
    state = b_in.shape[1]
    experts, rows, lanes = send.shape
    capacity = (rows - 2 * PIECE) // 2

    joined[0:RIM, :] = rim[...].astype(F32)
    joined[RIM:, 0:width] = x_in[...].astype(F32)
    joined[RIM:, width : width + state] = b_in[...].astype(F32)
    joined[RIM:, width + state :] = c_in[...].astype(F32)

    def filtered(first, size, taps_ref):
        taps = taps_ref[...].astype(F32)
        total = None
        for j in range(taps.shape[0]):
            start = RIM - taps.shape[0] + 1 + j
            term = taps[j : j + 1] * joined[start : start + count, first : first + size]
            total = term if total is None else total + term
        return silu(total)

    x = filtered(0, width, x_taps)
    b = filtered(width, state, b_taps).astype(BF16)
    c = filtered(width + state, state, c_taps).astype(BF16)
    x_out[...] = x
    b_out[...] = b
    c_out[...] = c

    def per_head(values):
        head = iota(strides.shape, 0)
        wide = jnp.full(strides.shape, values[0], F32)
        for k in range(1, strides.shape[0]):
            wide = jnp.where(head == k, values[k], wide)
        return wide

    raw = strides[...] + per_head(offset)
    step = jnp.maximum(raw, 0.0) + jnp.log1p(jnp.exp(-jnp.abs(raw)))
    total = -jnp.exp(per_head(speed)) * step + extra[...]
    both = jnp.concatenate([total, step], axis=0)
    lane = iota(both.shape, 1)
    shift = 1
    while shift < count:
        moved = jnp.where((lane >= shift), pltpu.roll(both, shift, axis=1), 0.0)
        both = jnp.where(iota(both.shape, 0) < 4, both + moved, both)
        shift *= 2
    columns = both.T
    rows_out[...] = both
    columns_out[...] = columns
    running, step_column = columns[:, 0:4], columns[:, 4:8]
    last = columns[count - 1 : count, 0:4]
    weight = step_column * jnp.exp(last - running)
    weighted = (x * spread(weight, HEAD_DIM)).astype(BF16)
    end_state = dot(weighted, b, (0, 0)).astype(BF16)
    high = last.astype(BF16).astype(F32)
    low = last - high
    half = iota((PIECE, lanes), 1) < lanes // 2
    for e in range(experts):
        head = e * PIECE // HEAD_DIM
        mine = routed[e * capacity : (e + 1) * capacity, :]
        send[e, 0:capacity, :] = mine[:, 0:lanes]
        send[e, capacity : 2 * capacity, :] = mine[:, lanes:]
        send[e, rows - 2 * PIECE : rows - PIECE, :] = end_state[e * PIECE : (e + 1) * PIECE]
        send[e, rows - PIECE :, :] = jnp.where(
            half, high[:, head : head + 1], low[:, head : head + 1]
        ).astype(BF16)


def enter_body(got, enter):
    sources, rows, lanes = got.shape
    size = sources * PIECE
    piece = got[:, rows - 2 * PIECE : rows - PIECE, :].reshape(size, lanes)
    logs = got[:, rows - PIECE :, :].reshape(size, lanes).astype(F32)
    logs = logs[:, 0:1] + logs[:, lanes // 2 : lanes // 2 + 1]
    row, column = iota((size, size), 0), iota((size, size), 1)
    before = column // PIECE < row // PIECE
    mean = jnp.where(before, 1.0 / PIECE, 0.0).astype(BF16)
    wide = jnp.broadcast_to(logs, (size, lanes))
    high = wide.astype(BF16)
    mid = (wide - high.astype(F32)).astype(BF16)
    low = (wide - high.astype(F32) - mid.astype(F32)).astype(BF16)
    earlier = dot(mean, high) + dot(mean, mid) + dot(mean, low)
    through = (earlier + wide).T[0:1, :]
    keep = before & (column % PIECE == row % PIECE)
    gap = jnp.where(keep, earlier[:, 0:1] - through, 0.0)
    decay = jnp.where(keep, jnp.exp(gap), 0.0)
    decay_high = decay.astype(BF16)
    decay_low = (decay - decay_high.astype(F32)).astype(BF16)
    result = dot(decay_high, piece) + dot(decay_low, piece)
    enter[...] = result.astype(BF16).reshape(sources, PIECE, lanes)


def inside_body(x_ref, b_ref, c_ref, columns, rows, bypass, out):
    count = x_ref.shape[0]
    scores = dot(c_ref[...], b_ref[...], (1, 1))
    causal = iota((count, count), 0) >= iota((count, count), 1)
    for head in range(4):
        part = slice(head * HEAD_DIM, (head + 1) * HEAD_DIM)
        gap = columns[:, head : head + 1] - rows[head : head + 1, :]
        weights = jnp.where(causal, jnp.exp(jnp.where(causal, gap, 0.0)), 0.0)
        x = x_ref[:, part]
        scaled = (x * columns[:, 4 + head : 5 + head]).astype(BF16)
        inside = dot((scores * weights).astype(BF16), scaled)
        out[:, part] = inside + bypass[head] * x


def finish_body(place, y, c, columns, enter, valve, gain, result, mine, other, normed):
    carried = dot(c[...], enter[...], (1, 1))
    carried = carried * spread(jnp.exp(columns[:, 0:4]), HEAD_DIM)
    gated = (y[...] + carried) * silu(valve[...].astype(F32))
    scale = lax.rsqrt(jnp.mean(gated * gated, axis=1, keepdims=True) + NORM_EPS)
    normed[...] = gated * scale * jnp.concatenate([gain[0:1, :], gain[1:2, :]], axis=1)
    chips, size, lanes = mine.shape
    width = result.shape[1]
    rows = size * lanes // width
    for target, core in ((mine, place[0]), (other, 1 - place[0])):
        parts = []
        for k in range(chips):
            at = (2 * ((place[1] + k) % chips) + core) * rows
            parts.append(normed[pl.ds(pl.multiple_of(at, rows), rows), :])
        left = jnp.concatenate(parts, axis=0).astype(BF16)
        block = 512
        for first in range(0, width, block):
            product = dot(left, result[:, first : first + block]).astype(BF16)
            for k in range(chips):
                for j in range(block // lanes):
                    at = (first // lanes + j) * rows
                    target[k, at : at + rows, :] = product[
                        k * rows : (k + 1) * rows, j * lanes : (j + 1) * lanes
                    ]


def joined_rows(piece, at, capacity):
    left = piece[at, 0:capacity, :]
    right = piece[at, capacity : 2 * capacity, :]
    rows, lanes = left.shape[0] * capacity, left.shape[2]
    return jnp.concatenate([left.reshape(rows, lanes), right.reshape(rows, lanes)], axis=1)


SOURCE_BLOCK = 8


def sums_body(which, first, final, place, *refs):
    refs = list(refs)
    before = [] if first else [refs.pop(0), refs.pop(0)]
    pieces = [refs.pop(0) for _ in which]
    valve, expand, *outs = refs
    sources = pieces[0].shape[0]
    capacity, size = pieces[0].shape[1] // 2, 2 * pieces[0].shape[2]
    count = SOURCE_BLOCK * capacity

    def step(i, _):
        at = pl.ds(i * SOURCE_BLOCK, SOURCE_BLOCK)
        out = pl.ds(pl.multiple_of(i * count, count), count)
        total = [ref[out, :] for ref in before]
        for (other, shift), piece in zip(which, pieces):
            core = 1 - place[0] if other else place[0]
            row = core * (4 * size) + (place[1] + shift) % 4 * size
            rows = pl.ds(pl.multiple_of(row, size), size)
            x = joined_rows(piece, at, capacity)
            more = [dot(x, matrix[rows, :]) for matrix in (valve, expand)]
            total = [t + m for t, m in zip(total, more)] if total else more
        if final:
            outs[0][out, :] = (silu(total[0]) * total[1]).astype(BF16)
        else:
            outs[0][out, :], outs[1][out, :] = total
        return 0

    lax.fori_loop(0, sources // SOURCE_BLOCK, step, 0)


def split_body(place, contract, keep, give):
    chips = keep.shape[1] // 128
    for k in range(chips):
        at = slice(k * 128, (k + 1) * 128)
        base = 2 * ((place[1] + k) % chips)
        for target, core in ((keep, place[0]), (give, 1 - place[0])):
            target[:, at] = contract[:, pl.ds(pl.multiple_of((base + core) * 128, 128), 128)]


def down_body(hidden, hidden_far, keep, keep_far, mine, other, right, left, across, stay):
    chips = keep.shape[1] // 128
    total = hidden.shape[0]
    block = total // 2
    homes = {
        0: (stay, 0), 1: (right, 0), 2: (stay, 1), 3: (right, 1),
        4: (across, 0), 5: (left, 1), 6: (stay, 2), 7: (left, 0),
    }

    def step(i, _):
        at = pl.ds(pl.multiple_of(i * block, block), block)
        near, far = hidden[at, :], hidden_far[at, :]
        for k in range(0, chips, 2):
            columns = slice(k * 128, (k + 2) * 128)
            product = dot(near, keep[:, columns]) + dot(far, keep_far[:, columns])
            for j in range(2):
                home, slot = homes[k + j]
                home[slot, at, :] = product[:, j * 128 : (j + 1) * 128].astype(BF16)
        return 0

    for k in range(chips):
        home, slot = homes[k]
        home[slot, total:, :] = (mine[k].astype(F32) + other[k].astype(F32)).astype(BF16)
    lax.fori_loop(0, total // block, step, 0)


def rim_body(x, b, c, out, done):
    first, copies = 0, []
    for k, part in enumerate((x, b, c)):
        size = part.shape[1]
        copy = pltpu.make_async_copy(
            part.at[pl.ds(part.shape[0] - RIM, RIM), :],
            out.at[:, pl.ds(first, size)],
            done.at[k],
        )
        copy.start()
        copies.append(copy)
        first += size
    for copy in copies:
        copy.wait()


def last_rows(*parts):
    width = sum(part.shape[1] for part in parts)
    return pl.pallas_call(
        rim_body,
        out_shape=shaped(RIM, width),
        in_specs=[pl.BlockSpec(memory_space=pltpu.HBM)] * len(parts),
        out_specs=VMEM,
        scratch_shapes=[pltpu.SemaphoreType.DMA((len(parts),))],
        compiler_params=pltpu.CompilerParams(vmem_limit_bytes=1 << 20),
    )(*parts)


def merge_body(place, stay, from_left, from_right, from_across, so_far, up_two, down_two):
    far = from_across[0].astype(F32)
    core = jnp.full((1, 1), place[0])
    so_far[...] = (
        stay[0].astype(F32) + from_left[0].astype(F32) + from_right[0].astype(F32)
    )
    up = stay[1].astype(F32) + from_left[1].astype(F32) + jnp.where(core == 0, far, 0.0)
    down = stay[2].astype(F32) + from_right[1].astype(F32) + jnp.where(core == 1, far, 0.0)
    up_two[...] = up.astype(BF16)
    down_two[...] = down.astype(BF16)


def total_body(so_far, from_up, from_down, out, rows_out):
    total = so_far[...] + from_up[...].astype(F32) + from_down[...].astype(F32)
    total = total.astype(BF16)
    count, lanes = out.shape
    rows, width = rows_out.shape
    out[...] = total[0:count]
    for j in range(width // lanes):
        first = count + j * rows
        rows_out[:, j * lanes : (j + 1) * lanes] = total[first : first + rows]


def combine_body(got, slots, coefs, out):
    sources, capacity, lanes = got.shape
    rows = got[...].reshape(sources * capacity, lanes)
    slot_ids = iota((rows.shape[0], slots.shape[1]), 0)
    padded = jnp.concatenate([coefs[...]] * (8 // TOPK), axis=0)
    columns = padded.T
    total = None
    for k in range(TOPK):
        chosen = (slot_ids == slots[k : k + 1, :]).astype(F32).astype(BF16)
        term = dot(chosen, rows, (0, 0)) * columns[:, k : k + 1]
        total = term if total is None else total + term
    out[...] = total.astype(BF16)


def local(
    blender_incoming_features,
    entry_latent_matrix,
    exit_latent_matrix,
    unactivated_valve,
    presoftplus_strides,
    extra_attenuation,
    incoming_feature_kernel,
    entry_latent_kernel,
    exit_latent_kernel,
    stride_offset_vector,
    attenuation_speed_exponent,
    bypass_coef_vector,
    cluster_rescale_coefs,
    blender_result_matrix,
    latter_microbatch_activations,
    specialist_rescale_coefs,
    specialist_valve_matrix,
    specialist_expand_matrix,
    specialist_contract_matrix,
    specialist_picks,
    selected_specialist_coefs,
):
    ep_count, chips = lax.axis_size(EP), lax.axis_size("tp_0")
    chip, core = lax.axis_index("tp_0"), lax.axis_index("tp_1")
    count, width = blender_incoming_features.shape
    state = entry_latent_matrix.shape[1]
    token_count, model_width = latter_microbatch_activations.shape
    capacity = 3 * token_count * TOPK // (2 * ep_count)
    lanes = model_width // lax.axis_size(TP)
    total_rows = ep_count * capacity
    place = jnp.stack([core, chip])
    valve = specialist_valve_matrix.reshape(model_width, -1)
    expand = specialist_expand_matrix.reshape(model_width, -1)
    contract = specialist_contract_matrix.reshape(-1, model_width)
    hidden_width = valve.shape[1]

    def permuted(x, axis, pairs):
        return lax.ppermute(x, axis, pairs)

    def around(x, distance):
        return permuted(x, "tp_0", [(i, (i + distance) % chips) for i in range(chips)])

    def across(x):
        pairs = []
        for i in range(chips):
            pairs.append((2 * i, 2 * ((i + 2) % chips)))
            pairs.append((2 * i + 1, 2 * ((i - 2) % chips) + 1))
        return permuted(x, TP, pairs)

    def partner(x):
        return permuted(x, "tp_1", [(0, 1), (1, 0)])

    def exchanged(x, axis):
        return lax.all_to_all(x, axis, 0, 0, tiled=True)

    rim = last_rows(blender_incoming_features, entry_latent_matrix, exit_latent_matrix)
    rim = permuted(rim, EP, [(i, i + 1) for i in range(ep_count - 1)])
    keep, give = call(
        split_body,
        (shaped(hidden_width, model_width // 2),) * 2,
        (place, contract),
        1 << 30,
        8,
        smem=1,
    )
    keep_far = partner(give)
    routed, slots = call(
        functools.partial(route_body, ep_count),
        (shaped(total_rows, 2 * lanes), shaped(TOPK, token_count, dtype=jnp.int32)),
        (
            (core * chips + chip % 4 * 2).reshape(1),
            latter_microbatch_activations,
            specialist_rescale_coefs.astype(F32).reshape(-1, lanes),
            specialist_picks.T,
        ),
        1 << 30,
        16,
        smem=1,
    )
    send, x, b, c, columns, rows = call(
        filter_body,
        (
            shaped(ep_count, 2 * capacity + 2 * PIECE, lanes),
            shaped(count, width, dtype=F32),
            shaped(count, state),
            shaped(count, state),
            shaped(count, 8, dtype=F32),
            shaped(8, count, dtype=F32),
        ),
        (
            stride_offset_vector,
            attenuation_speed_exponent,
            routed,
            blender_incoming_features,
            entry_latent_matrix,
            exit_latent_matrix,
            rim,
            incoming_feature_kernel,
            entry_latent_kernel,
            exit_latent_kernel,
            presoftplus_strides.T,
            extra_attenuation.T,
        ),
        1 << 30,
        10,
        scratch=(pltpu.VMEM((RIM + count, width + 2 * state), F32),),
        smem=2,
    )
    got = exchanged(send, EP)
    y = inside(bypass_coef_vector, x, b, c, columns, rows)

    own = got[:, 0 : 2 * capacity, :]
    left, right = around(own, 1), around(own, -1)
    beyond = across(own)
    far_own, far_left = partner(own), partner(left)
    far_right, far_beyond = partner(right), partner(beyond)

    def sums(which, before, pieces, final=False):
        first = before is None
        return call(
            functools.partial(sums_body, which, first, final),
            shaped(total_rows, hidden_width)
            if final
            else (shaped(total_rows, hidden_width, dtype=F32),) * 2,
            (place, *(() if first else before), *pieces, valve, expand),
            1 << 31,
            12,
            smem=1,
        )

    partial = sums(((0, 0), (0, 3), (0, 1)), None, (own, left, right))
    partial = sums(
        ((0, 2), (1, 0), (1, 3), (1, 1)), partial, (beyond, far_own, far_left, far_right)
    )
    hidden = sums(((1, 2),), partial, (far_beyond,), True)
    enter = call(enter_body, shaped(ep_count, PIECE, lanes), (got,), 1 << 30, 8)
    enter = exchanged(enter, EP).reshape(width, state)
    row_block = count * model_width // (2 * chips * lanes)
    mine_a, other_a = call(
        finish_body,
        (shaped(chips, row_block, lanes),) * 2,
        (
            place,
            y,
            c,
            columns,
            enter,
            unactivated_valve,
            cluster_rescale_coefs.astype(F32).reshape(-1, 128),
            blender_result_matrix,
        ),
        1 << 31,
        10,
        scratch=(pltpu.VMEM((count, width), F32),),
        smem=1,
    )
    other_a = partner(other_a)
    hidden_far = partner(hidden)
    all_rows = total_rows + row_block
    to_right, to_left, to_across, stay = call(
        down_body,
        tuple(shaped(k, all_rows, lanes) for k in (2, 2, 1, 3)),
        (hidden, hidden_far, keep, keep_far, mine_a, other_a),
        1 << 31,
        14,
    )
    from_left, from_right = around(to_right, 1), around(to_left, -1)
    from_across = across(to_across)
    so_far, up_two, down_two = call(
        merge_body,
        (
            shaped(all_rows, lanes, dtype=F32),
            shaped(all_rows, lanes),
            shaped(all_rows, lanes),
        ),
        (place, stay, from_left, from_right, from_across),
        1 << 29,
        6,
        smem=1,
    )
    from_up, from_down = around(up_two, 2), around(down_two, -2)
    summed, mixed_a = call(
        total_body,
        (shaped(total_rows, lanes), shaped(count // (2 * chips), model_width)),
        (so_far, from_up, from_down),
        1 << 29,
        4,
    )
    returned = exchanged(summed.reshape(ep_count, capacity, lanes), EP)
    mixed_b = call(
        combine_body,
        shaped(token_count, lanes),
        (returned, slots, selected_specialist_coefs.T),
        1 << 28,
        8,
    )
    return (mixed_a, mixed_b)


def inside(bypass, x, b, c, columns, rows):
    def body(bypass, x, b, c, columns, rows, out):
        inside_body(x, b, c, columns, rows, bypass, out)

    return call(
        body, shaped(*x.shape, dtype=F32), (bypass, x, b, c, columns, rows), 1 << 31, 8, smem=1
    )


def solution(mesh):
    split = Mesh(mesh.devices.reshape(8, 4, 8, 2), ("ep_0", "ep_1", "tp_0", "tp_1"))
    in_specs = (
        P(EP, TP),
        P(EP, TP),
        P(EP, TP),
        P(EP, TP),
        P(EP, TP),
        P(EP, TP),
        P(None, TP),
        P(None, TP),
        P(None, TP),
        P(TP),
        P(TP),
        P(TP),
        P(TP),
        P(TP, None),
        P(EP, None),
        P(),
        P(EP, None, TP),
        P(EP, None, TP),
        P(EP, TP, None),
        P(EP, None),
        P(EP, None),
    )
    out_specs = (P(EP_TP, None), P(EP, TP))

    return jax.shard_map(local, mesh=split, in_specs=in_specs, out_specs=out_specs, check_vma=False)
```

```python
import functools

import jax
import jax.numpy as jnp
from jax import lax
from jax.experimental import pallas as pl
from jax.experimental.pallas import tpu as pltpu
from jax.sharding import Mesh
from jax.sharding import PartitionSpec as P


HEAD_DIM = 64
TOPK = 2
EP = ("ep_0", "ep_1")
TP = ("tp_0", "tp_1")
EP_TP = ("ep_0", "ep_1", "tp_0", "tp_1")
RIM = 8
PIECE = 8

NORM_EPS = 1e-06
F32 = jnp.float32
BF16 = jnp.bfloat16
VMEM = pl.BlockSpec(memory_space=pltpu.VMEM)
SMEM = pl.BlockSpec(memory_space=pltpu.SMEM)


def call(body, outs, ins, flops, room, scratch=(), smem=0):
    return pl.pallas_call(
        body,
        out_shape=outs,
        in_specs=[SMEM] * smem + [VMEM] * (len(ins) - smem),
        out_specs=jax.tree.map(lambda _: VMEM, outs),
        scratch_shapes=scratch,
        cost_estimate=pl.CostEstimate(flops=flops, bytes_accessed=1 << 20, transcendentals=0),
        compiler_params=pltpu.CompilerParams(vmem_limit_bytes=room << 20 if room else None),
    )(*ins)


def shaped(*shape, dtype=BF16):
    return jax.ShapeDtypeStruct(shape, dtype)


def iota(shape, dim):
    return lax.broadcasted_iota(jnp.int32, shape, dim)


def silu(v):
    return v * jax.nn.sigmoid(v)


def dot(a, b, contract=(1, 0)):
    return lax.dot_general(
        a, b, (((contract[0],), (contract[1],)), ((), ())), preferred_element_type=F32
    )


def spread(columns, width):
    lane_head = iota((columns.shape[0], 4 * width), 1) // width
    wide = columns[:, 0:1]
    for head in range(1, 4):
        wide = jnp.where(lane_head == head, columns[:, head : head + 1], wide)
    return wide


def route_body(experts, place, tokens, token_gain, picks, routed, slots_out):
    lanes = token_gain.shape[1]
    total_rows, token_count = routed.shape[0], tokens.shape[0]
    capacity = total_rows // experts
    data = tokens[...].astype(F32)
    scale = lax.rsqrt(jnp.mean(data * data, axis=1, keepdims=True) + NORM_EPS)
    first = pl.multiple_of(place[0] * lanes, lanes)
    chosen = tokens[:, pl.ds(first, 2 * lanes)].astype(F32)
    gain = jnp.concatenate([token_gain[pl.ds(place[0] + k, 1), :] for k in range(2)], axis=1)
    chosen = (chosen * scale * gain).astype(BF16)
    expert = iota((experts, token_count), 0)
    earlier = (
        iota((token_count, token_count), 0) < iota((token_count, token_count), 1)
    ).astype(BF16)
    base = jnp.zeros((experts, 1), F32)
    slot_ids = iota((total_rows, token_count), 0)
    placing = None
    for k in range(TOPK):
        pick = picks[k : k + 1, :]
        named = (expert == pick).astype(F32)
        rank = base + dot(named.astype(BF16), earlier)
        rank = jnp.sum(named * rank, axis=0, keepdims=True)
        slot = pick * capacity + rank.astype(jnp.int32)
        slots_out[k : k + 1, :] = slot
        base = base + jnp.sum(named, axis=1, keepdims=True)
        hit = slot_ids == slot
        placing = hit if placing is None else placing | hit
    routed[...] = dot(placing.astype(F32).astype(BF16), chosen).astype(BF16)


def filter_body(
    offset,
    speed,
    routed,
    x_in,
    b_in,
    c_in,
    rim,
    x_taps,
    b_taps,
    c_taps,
    strides,
    extra,
    send,
    x_out,
    b_out,
    c_out,
    columns_out,
    rows_out,
    joined,
):
    count, width = x_in.shape
    state = b_in.shape[1]
    experts, rows, lanes = send.shape
    capacity = (rows - 2 * PIECE) // 2

    joined[0:RIM, :] = rim[...].astype(F32)
    joined[RIM:, 0:width] = x_in[...].astype(F32)
    joined[RIM:, width : width + state] = b_in[...].astype(F32)
    joined[RIM:, width + state :] = c_in[...].astype(F32)

    def filtered(first, size, taps_ref):
        taps = taps_ref[...].astype(F32)
        total = None
        for j in range(taps.shape[0]):
            start = RIM - taps.shape[0] + 1 + j
            term = taps[j : j + 1] * joined[start : start + count, first : first + size]
            total = term if total is None else total + term
        return silu(total)

    x = filtered(0, width, x_taps)
    b = filtered(width, state, b_taps).astype(BF16)
    c = filtered(width + state, state, c_taps).astype(BF16)
    x_out[...] = x
    b_out[...] = b
    c_out[...] = c

    def per_head(values):
        head = iota(strides.shape, 0)
        wide = jnp.full(strides.shape, values[0], F32)
        for k in range(1, strides.shape[0]):
            wide = jnp.where(head == k, values[k], wide)
        return wide

    raw = strides[...] + per_head(offset)
    step = jnp.maximum(raw, 0.0) + jnp.log1p(jnp.exp(-jnp.abs(raw)))
    total = -jnp.exp(per_head(speed)) * step + extra[...]
    both = jnp.concatenate([total, step], axis=0)
    lane = iota(both.shape, 1)
    shift = 1
    while shift < count:
        moved = jnp.where((lane >= shift), pltpu.roll(both, shift, axis=1), 0.0)
        both = jnp.where(iota(both.shape, 0) < 4, both + moved, both)
        shift *= 2
    columns = both.T
    rows_out[...] = both
    columns_out[...] = columns
    running, step_column = columns[:, 0:4], columns[:, 4:8]
    last = columns[count - 1 : count, 0:4]
    weight = step_column * jnp.exp(last - running)
    weighted = (x * spread(weight, HEAD_DIM)).astype(BF16)
    end_state = dot(weighted, b, (0, 0)).astype(BF16)
    high = last.astype(BF16).astype(F32)
    low = last - high
    half = iota((PIECE, lanes), 1) < lanes // 2
    for e in range(experts):
        head = e * PIECE // HEAD_DIM
        mine = routed[e * capacity : (e + 1) * capacity, :]
        send[e, 0:capacity, :] = mine[:, 0:lanes]
        send[e, capacity : 2 * capacity, :] = mine[:, lanes:]
        send[e, rows - 2 * PIECE : rows - PIECE, :] = end_state[e * PIECE : (e + 1) * PIECE]
        send[e, rows - PIECE :, :] = jnp.where(
            half, high[:, head : head + 1], low[:, head : head + 1]
        ).astype(BF16)


def enter_body(got, enter):
    sources, rows, lanes = got.shape
    size = sources * PIECE
    piece = got[:, rows - 2 * PIECE : rows - PIECE, :].reshape(size, lanes)
    logs = got[:, rows - PIECE :, :].reshape(size, lanes).astype(F32)
    logs = logs[:, 0:1] + logs[:, lanes // 2 : lanes // 2 + 1]
    row, column = iota((size, size), 0), iota((size, size), 1)
    before = column // PIECE < row // PIECE
    mean = jnp.where(before, 1.0 / PIECE, 0.0).astype(BF16)
    wide = jnp.broadcast_to(logs, (size, lanes))
    high = wide.astype(BF16)
    mid = (wide - high.astype(F32)).astype(BF16)
    low = (wide - high.astype(F32) - mid.astype(F32)).astype(BF16)
    earlier = dot(mean, high) + dot(mean, mid) + dot(mean, low)
    through = (earlier + wide).T[0:1, :]
    keep = before & (column % PIECE == row % PIECE)
    gap = jnp.where(keep, earlier[:, 0:1] - through, 0.0)
    decay = jnp.where(keep, jnp.exp(gap), 0.0)
    decay_high = decay.astype(BF16)
    decay_low = (decay - decay_high.astype(F32)).astype(BF16)
    result = dot(decay_high, piece) + dot(decay_low, piece)
    enter[...] = result.astype(BF16).reshape(sources, PIECE, lanes)


def inside_body(x_ref, b_ref, c_ref, columns, rows, bypass, out):
    count = x_ref.shape[0]
    scores = dot(c_ref[...], b_ref[...], (1, 1))
    causal = iota((count, count), 0) >= iota((count, count), 1)
    for head in range(4):
        part = slice(head * HEAD_DIM, (head + 1) * HEAD_DIM)
        gap = columns[:, head : head + 1] - rows[head : head + 1, :]
        weights = jnp.where(causal, jnp.exp(jnp.where(causal, gap, 0.0)), 0.0)
        x = x_ref[:, part]
        scaled = (x * columns[:, 4 + head : 5 + head]).astype(BF16)
        inside = dot((scores * weights).astype(BF16), scaled)
        out[:, part] = inside + bypass[head] * x


def finish_body(place, y, c, columns, enter, valve, gain, mine, other, normed):
    carried = dot(c[...], enter[...], (1, 1))
    carried = carried * spread(jnp.exp(columns[:, 0:4]), HEAD_DIM)
    gated = (y[...] + carried) * silu(valve[...].astype(F32))
    scale = lax.rsqrt(jnp.mean(gated * gated, axis=1, keepdims=True) + NORM_EPS)
    normed[...] = gated * scale * jnp.concatenate([gain[0:1, :], gain[1:2, :]], axis=1)
    chips = 8
    rows = mine.shape[0] // chips
    for target, core in ((mine, place[0]), (other, 1 - place[0])):
        parts = []
        for k in range(chips):
            at = (2 * ((place[1] + k) % chips) + core) * rows
            parts.append(normed[pl.ds(pl.multiple_of(at, rows), rows), :])
        target[...] = jnp.concatenate(parts, axis=0).astype(BF16)


def joined_rows(piece, at, capacity):
    left = piece[at, 0:capacity, :]
    right = piece[at, capacity : 2 * capacity, :]
    rows, lanes = left.shape[0] * capacity, left.shape[2]
    return jnp.concatenate([left.reshape(rows, lanes), right.reshape(rows, lanes)], axis=1)


SOURCE_BLOCK = 8


def feature_sums(pieces, at, capacity, rows_of, gates, ups):
    gate = up = None
    for shift, piece in zip((0, 3, 1, 2), pieces):
        x = joined_rows(piece, at, capacity)
        rows = rows_of(shift)
        more = dot(x, gates[rows[0], :]), dot(x, ups[rows[1], :])
        gate, up = more if gate is None else (gate + more[0], up + more[1])
    return gate, up


def theirs_body(place, own, left, right, across, weights, out):
    sources, capacity = own.shape[0], own.shape[1] // 2
    size = 2 * own.shape[2]
    count = SOURCE_BLOCK * capacity

    def rows_of(shift):
        first = (place[1] + shift) % 4 * size
        return [pl.ds(pl.multiple_of(first + 4 * size * k, size), size) for k in range(2)]

    def step(i, _):
        at = pl.ds(i * SOURCE_BLOCK, SOURCE_BLOCK)
        to = pl.ds(pl.multiple_of(i * count, count), count)
        gate, up = feature_sums(
            (own, left, right, across), at, capacity, rows_of, weights, weights
        )
        width = gate.shape[1]
        out[to, 0:width] = gate.astype(BF16)
        out[to, width:] = up.astype(BF16)
        return 0

    lax.fori_loop(0, sources // SOURCE_BLOCK, step, 0)


def ours_body(place, own, left, right, across, valve, expand, other, rows, out):
    sources, capacity = own.shape[0], own.shape[1] // 2
    size = 2 * own.shape[2]
    count = SOURCE_BLOCK * capacity

    def rows_of(shift):
        first = place[0] * (4 * size) + (place[1] + shift) % 4 * size
        return [pl.ds(pl.multiple_of(first, size), size)] * 2

    def step(i, _):
        at = pl.ds(i * SOURCE_BLOCK, SOURCE_BLOCK)
        to = pl.ds(pl.multiple_of(i * count, count), count)
        gate, up = feature_sums((own, left, right, across), at, capacity, rows_of, valve, expand)
        width = gate.shape[1]
        gate = gate + other[to, 0:width].astype(F32)
        up = up + other[to, width:].astype(F32)
        out[to, :] = (silu(gate) * up).astype(BF16)
        return 0

    lax.fori_loop(0, sources // SOURCE_BLOCK, step, 0)
    out[sources * capacity :, :] = rows[...]


def split_body(place, valve, expand, contract, keep, give):
    half = valve.shape[0] // 2
    theirs = pl.ds(pl.multiple_of((1 - place[0]) * half, half), half)
    give[0:half, :] = valve[theirs, :]
    give[half : 2 * half, :] = expand[theirs, :]
    depth = contract.shape[0]
    chips = 8
    for k in range(chips):
        base = 2 * ((place[1] + k) % chips)
        row, lane = k // 2 * depth, k % 2 * 128
        for target, core, first in ((keep, place[0], 0), (give, 1 - place[0], 2 * half)):
            target[first + row : first + row + depth, lane : lane + 128] = contract[
                :, pl.ds(pl.multiple_of((base + core) * 128, 128), 128)
            ]


def down_body(own, far, rows, keep, weights, result, result_far, right, left, across, stay):
    chips, depth = 8, own.shape[1]
    count = rows.shape[0]
    total = own.shape[0] - count
    far_first = weights.shape[0] - keep.shape[0]
    block = total // 2
    homes = {
        0: (stay, 0), 1: (right, 0), 2: (stay, 1), 3: (right, 1),
        4: (across, 0), 5: (left, 1), 6: (stay, 2), 7: (left, 0),
    }

    def step(i, _):
        at = pl.ds(pl.multiple_of(i * block, block), block)
        near, beyond = own[at, :], far[at, :]
        for k in range(0, chips, 2):
            row = k // 2 * depth
            product = dot(near, keep[row : row + depth, :]) + dot(
                beyond, weights[far_first + row : far_first + row + depth, :]
            )
            for j in range(2):
                home, slot = homes[k + j]
                home[slot, at, :] = product[:, j * 128 : (j + 1) * 128].astype(BF16)
        return 0

    lax.fori_loop(0, total // block, step, 0)
    near, beyond = rows[...], far[total:, :]
    each, wide = count // chips, 512
    for first in range(0, result.shape[1], wide):
        columns = slice(first, first + wide)
        product = dot(near, result[:, columns]) + dot(beyond, result_far[:, columns])
        product = product.astype(BF16)
        for k in range(chips):
            home, slot = homes[k]
            for j in range(wide // 128):
                to = total + (first // 128 + j) * each
                home[slot, to : to + each, :] = product[
                    k * each : (k + 1) * each, j * 128 : (j + 1) * 128
                ]


def rim_body(x, b, c, out, done):
    first, copies = 0, []
    for k, part in enumerate((x, b, c)):
        size = part.shape[1]
        copy = pltpu.make_async_copy(
            part.at[pl.ds(part.shape[0] - RIM, RIM), :],
            out.at[:, pl.ds(first, size)],
            done.at[k],
        )
        copy.start()
        copies.append(copy)
        first += size
    for copy in copies:
        copy.wait()


def last_rows(*parts):
    width = sum(part.shape[1] for part in parts)
    return pl.pallas_call(
        rim_body,
        out_shape=shaped(RIM, width),
        in_specs=[pl.BlockSpec(memory_space=pltpu.HBM)] * len(parts),
        out_specs=VMEM,
        scratch_shapes=[pltpu.SemaphoreType.DMA((len(parts),))],
    )(*parts)


def merge_body(place, stay, from_left, from_right, from_across, so_far, up_two, down_two):
    far = from_across[0].astype(F32)
    core = jnp.full((1, 1), place[0])
    so_far[...] = (
        stay[0].astype(F32) + from_left[0].astype(F32) + from_right[0].astype(F32)
    )
    up = stay[1].astype(F32) + from_left[1].astype(F32) + jnp.where(core == 0, far, 0.0)
    down = stay[2].astype(F32) + from_right[1].astype(F32) + jnp.where(core == 1, far, 0.0)
    up_two[...] = up.astype(BF16)
    down_two[...] = down.astype(BF16)


def total_body(so_far, from_up, from_down, out, rows_out):
    total = so_far[...] + from_up[...].astype(F32) + from_down[...].astype(F32)
    total = total.astype(BF16)
    count, lanes = out.shape
    rows, width = rows_out.shape
    out[...] = total[0:count]
    for j in range(width // lanes):
        first = count + j * rows
        rows_out[:, j * lanes : (j + 1) * lanes] = total[first : first + rows]


def combine_body(got, slots, coefs, out):
    sources, capacity, lanes = got.shape
    rows = got[...].reshape(sources * capacity, lanes)
    slot_ids = iota((rows.shape[0], slots.shape[1]), 0)
    padded = jnp.concatenate([coefs[...]] * (8 // TOPK), axis=0)
    columns = padded.T
    total = None
    for k in range(TOPK):
        chosen = (slot_ids == slots[k : k + 1, :]).astype(F32).astype(BF16)
        term = dot(chosen, rows, (0, 0)) * columns[:, k : k + 1]
        total = term if total is None else total + term
    out[...] = total.astype(BF16)


def local(
    blender_incoming_features,
    entry_latent_matrix,
    exit_latent_matrix,
    unactivated_valve,
    presoftplus_strides,
    extra_attenuation,
    incoming_feature_kernel,
    entry_latent_kernel,
    exit_latent_kernel,
    stride_offset_vector,
    attenuation_speed_exponent,
    bypass_coef_vector,
    cluster_rescale_coefs,
    blender_result_matrix,
    latter_microbatch_activations,
    specialist_rescale_coefs,
    specialist_valve_matrix,
    specialist_expand_matrix,
    specialist_contract_matrix,
    specialist_picks,
    selected_specialist_coefs,
):
    ep_count, chips = lax.axis_size(EP), lax.axis_size("tp_0")
    chip, core = lax.axis_index("tp_0"), lax.axis_index("tp_1")
    count, width = blender_incoming_features.shape
    state = entry_latent_matrix.shape[1]
    token_count, model_width = latter_microbatch_activations.shape
    capacity = 3 * token_count * TOPK // (2 * ep_count)
    lanes = model_width // lax.axis_size(TP)
    total_rows = ep_count * capacity
    place = jnp.stack([core, chip])
    valve = specialist_valve_matrix.reshape(model_width, -1)
    expand = specialist_expand_matrix.reshape(model_width, -1)
    contract = specialist_contract_matrix.reshape(-1, model_width)
    hidden_width = valve.shape[1]

    def around(x, distance):
        return lax.ppermute(x, "tp_0", [(i, (i + distance) % chips) for i in range(chips)])

    def across(x):
        pairs = []
        for i in range(chips):
            pairs.append((2 * i, 2 * ((i + 2) % chips)))
            pairs.append((2 * i + 1, 2 * ((i - 2) % chips) + 1))
        return lax.ppermute(x, TP, pairs)

    def partner(x):
        return lax.ppermute(x, "tp_1", [(0, 1), (1, 0)])

    def exchanged(x, axis):
        return lax.all_to_all(x, axis, 0, 0, tiled=True)

    rim = last_rows(blender_incoming_features, entry_latent_matrix, exit_latent_matrix)
    rim = lax.ppermute(rim, EP, [(i, i + 1) for i in range(ep_count - 1)])
    routed, slots = call(
        functools.partial(route_body, ep_count),
        (shaped(total_rows, 2 * lanes), shaped(TOPK, token_count, dtype=jnp.int32)),
        (
            (core * chips + chip % 4 * 2).reshape(1),
            latter_microbatch_activations,
            specialist_rescale_coefs.astype(F32).reshape(-1, lanes),
            specialist_picks.T,
        ),
        1 << 30,
        None,
        smem=1,
    )
    send, x, b, c, columns, rows = call(
        filter_body,
        (
            shaped(ep_count, 2 * capacity + 2 * PIECE, lanes),
            shaped(count, width, dtype=F32),
            shaped(count, state),
            shaped(count, state),
            shaped(count, 8, dtype=F32),
            shaped(8, count, dtype=F32),
        ),
        (
            stride_offset_vector,
            attenuation_speed_exponent,
            routed,
            blender_incoming_features,
            entry_latent_matrix,
            exit_latent_matrix,
            rim,
            incoming_feature_kernel,
            entry_latent_kernel,
            exit_latent_kernel,
            presoftplus_strides.T,
            extra_attenuation.T,
        ),
        1 << 30,
        None,
        scratch=(pltpu.VMEM((RIM + count, width + 2 * state), F32),),
        smem=2,
    )
    got = exchanged(send, EP)
    y = inside(bypass_coef_vector, x, b, c, columns, rows)

    half = model_width // 2
    keep, give = call(
        split_body,
        (shaped(half, hidden_width), shaped(3 * half, hidden_width)),
        (place, valve, expand, contract),
        1 << 30,
        None,
        smem=1,
    )
    weights_far = partner(give)
    result_far = partner(blender_result_matrix)

    own = got[:, 0 : 2 * capacity, :]
    beyond = across(own)
    left, right = around(own, 1), around(own, -1)
    pieces = (own, left, right, beyond)
    theirs = call(
        theirs_body,
        shaped(total_rows, 2 * hidden_width),
        (place, *pieces, weights_far),
        1 << 31,
        10,
        smem=1,
    )
    theirs = partner(theirs)

    enter = call(enter_body, shaped(ep_count, PIECE, lanes), (got,), 1 << 30, 8)
    enter = exchanged(enter, EP).reshape(width, state)
    row_count = count // 2
    mine_rows, other_rows = call(
        finish_body,
        (shaped(row_count, width),) * 2,
        (
            place,
            y,
            c,
            columns,
            enter,
            unactivated_valve,
            cluster_rescale_coefs.astype(F32).reshape(-1, 128),
        ),
        1 << 31,
        8,
        scratch=(pltpu.VMEM((count, width), F32),),
        smem=1,
    )
    ours = call(
        ours_body,
        shaped(total_rows + row_count, hidden_width),
        (place, *pieces, valve, expand, theirs, other_rows),
        1 << 31,
        10,
        smem=1,
    )
    ours_far = partner(ours)
    row_block = count * model_width // (2 * chips * lanes)
    all_rows = total_rows + row_block
    to_right, to_left, to_across, stay = call(
        down_body,
        tuple(shaped(k, all_rows, lanes) for k in (2, 2, 1, 3)),
        (ours, ours_far, mine_rows, keep, weights_far, blender_result_matrix, result_far),
        1 << 31,
        14,
    )
    from_left, from_right = around(to_right, 1), around(to_left, -1)
    from_across = across(to_across)
    so_far, up_two, down_two = call(
        merge_body,
        (
            shaped(all_rows, lanes, dtype=F32),
            shaped(all_rows, lanes),
            shaped(all_rows, lanes),
        ),
        (place, stay, from_left, from_right, from_across),
        1 << 29,
        6,
        smem=1,
    )
    from_up, from_down = around(up_two, 2), around(down_two, -2)
    summed, mixed_a = call(
        total_body,
        (shaped(total_rows, lanes), shaped(count // (2 * chips), model_width)),
        (so_far, from_up, from_down),
        1 << 29,
        4,
    )
    returned = exchanged(summed.reshape(ep_count, capacity, lanes), EP)
    mixed_b = call(
        combine_body,
        shaped(token_count, lanes),
        (returned, slots, selected_specialist_coefs.T),
        1 << 28,
        8,
    )
    return (mixed_a, mixed_b)


def inside(bypass, x, b, c, columns, rows):
    def body(bypass, x, b, c, columns, rows, out):
        inside_body(x, b, c, columns, rows, bypass, out)

    return call(
        body, shaped(*x.shape, dtype=F32), (bypass, x, b, c, columns, rows), 1 << 31, 8, smem=1
    )


def solution(mesh):
    split = Mesh(mesh.devices.reshape(8, 4, 8, 2), ("ep_0", "ep_1", "tp_0", "tp_1"))
    in_specs = (
        P(EP, TP),
        P(EP, TP),
        P(EP, TP),
        P(EP, TP),
        P(EP, TP),
        P(EP, TP),
        P(None, TP),
        P(None, TP),
        P(None, TP),
        P(TP),
        P(TP),
        P(TP),
        P(TP),
        P(TP, None),
        P(EP, None),
        P(),
        P(EP, None, TP),
        P(EP, None, TP),
        P(EP, TP, None),
        P(EP, None),
        P(EP, None),
    )
    out_specs = (P(EP_TP, None), P(EP, TP))

    return jax.shard_map(local, mesh=split, in_specs=in_specs, out_specs=out_specs, check_vma=False)
```

```python
import functools

import jax
import jax.numpy as jnp
from jax import lax
from jax.experimental import pallas as pl
from jax.experimental.pallas import tpu as pltpu
from jax.sharding import Mesh
from jax.sharding import PartitionSpec as P


HEAD_DIM = 64
TOPK = 2
EP = ("ep_0", "ep_1")
TP = ("tp_0", "tp_1")
EP_TP = ("ep_0", "ep_1", "tp_0", "tp_1")
RIM = 8
PIECE = 8
HOMES = (3, 5, 4, 6, 1, 7, 0, 2)

NORM_EPS = 1e-06
F32 = jnp.float32
BF16 = jnp.bfloat16
VMEM = pl.BlockSpec(memory_space=pltpu.VMEM)
SMEM = pl.BlockSpec(memory_space=pltpu.SMEM)


def call(body, outs, ins, flops, room, scratch=(), smem=0):
    return pl.pallas_call(
        body,
        out_shape=outs,
        in_specs=[SMEM] * smem + [VMEM] * (len(ins) - smem),
        out_specs=jax.tree.map(lambda _: VMEM, outs),
        scratch_shapes=scratch,
        cost_estimate=pl.CostEstimate(flops=flops, bytes_accessed=1 << 20, transcendentals=0),
        compiler_params=pltpu.CompilerParams(vmem_limit_bytes=room << 20 if room else None),
    )(*ins)


def placed(body):
    def run(core, chip, *refs):
        body((core[0], chip[0]), *refs)

    return run


def shaped(*shape, dtype=BF16):
    return jax.ShapeDtypeStruct(shape, dtype)


def iota(shape, dim):
    return lax.broadcasted_iota(jnp.int32, shape, dim)


def silu(v):
    return v * jax.nn.sigmoid(v)


def dot(a, b, contract=(1, 0)):
    return lax.dot_general(
        a, b, (((contract[0],), (contract[1],)), ((), ())), preferred_element_type=F32
    )


def spread(columns, width):
    lane_head = iota((columns.shape[0], 4 * width), 1) // width
    wide = columns[:, 0:1]
    for head in range(1, 4):
        wide = jnp.where(lane_head == head, columns[:, head : head + 1], wide)
    return wide


def route_body(experts, place, tokens, token_gain, picks, routed, slots_out):
    lanes = 128
    total_rows, token_count = routed.shape[0], tokens.shape[0]
    capacity = total_rows // experts
    data = tokens[...].astype(F32)
    scale = lax.rsqrt(jnp.mean(data * data, axis=1, keepdims=True) + NORM_EPS)
    first = pl.multiple_of(place[0] * (2 * lanes), 2 * lanes)
    chosen = tokens[:, pl.ds(first, 2 * lanes)].astype(F32)
    gain = token_gain[pl.ds(first, 2 * lanes)].astype(F32).reshape(1, 2 * lanes)
    chosen = (chosen * scale * gain).astype(BF16)
    expert = iota((experts, token_count), 0)
    earlier = (
        iota((token_count, token_count), 0) < iota((token_count, token_count), 1)
    ).astype(BF16)
    base = jnp.zeros((experts, 1), F32)
    slot_ids = iota((total_rows, token_count), 0)
    placing = None
    for k in range(TOPK):
        pick = picks[k : k + 1, :]
        named = (expert == pick).astype(F32)
        rank = base + dot(named.astype(BF16), earlier)
        rank = jnp.sum(named * rank, axis=0, keepdims=True)
        slot = pick * capacity + rank.astype(jnp.int32)
        slots_out[k : k + 1, :] = slot
        base = base + jnp.sum(named, axis=1, keepdims=True)
        hit = slot_ids == slot
        placing = hit if placing is None else placing | hit
    routed[...] = dot(placing.astype(F32).astype(BF16), chosen).astype(BF16)


def filter_body(
    offset,
    speed,
    routed,
    x_in,
    b_in,
    c_in,
    rim,
    x_taps,
    b_taps,
    c_taps,
    strides,
    extra,
    send,
    x_out,
    b_out,
    c_out,
    columns_out,
    rows_out,
    joined,
):
    count, width = x_in.shape
    state = b_in.shape[1]
    experts, rows, lanes = send.shape
    capacity = (rows - 2 * PIECE) // 2

    joined[0:RIM, :] = rim[...].astype(F32)
    joined[RIM:, 0:width] = x_in[...].astype(F32)
    joined[RIM:, width : width + state] = b_in[...].astype(F32)
    joined[RIM:, width + state :] = c_in[...].astype(F32)

    def filtered(first, size, taps_ref):
        taps = taps_ref[...].astype(F32)
        total = None
        for j in range(taps.shape[0]):
            start = RIM - taps.shape[0] + 1 + j
            term = taps[j : j + 1] * joined[start : start + count, first : first + size]
            total = term if total is None else total + term
        return silu(total)

    x = filtered(0, width, x_taps)
    b = filtered(width, state, b_taps).astype(BF16)
    c = filtered(width + state, state, c_taps).astype(BF16)
    x_out[...] = x
    b_out[...] = b
    c_out[...] = c

    def per_head(values):
        head = iota(strides.shape, 0)
        wide = jnp.full(strides.shape, values[0], F32)
        for k in range(1, strides.shape[0]):
            wide = jnp.where(head == k, values[k], wide)
        return wide

    raw = strides[...] + per_head(offset)
    step = jnp.maximum(raw, 0.0) + jnp.log1p(jnp.exp(-jnp.abs(raw)))
    total = -jnp.exp(per_head(speed)) * step + extra[...]
    both = jnp.concatenate([total, step], axis=0)
    lane = iota(both.shape, 1)
    shift = 1
    while shift < count:
        moved = jnp.where((lane >= shift), pltpu.roll(both, shift, axis=1), 0.0)
        both = jnp.where(iota(both.shape, 0) < 4, both + moved, both)
        shift *= 2
    columns = both.T
    rows_out[...] = both
    columns_out[...] = columns
    running, step_column = columns[:, 0:4], columns[:, 4:8]
    last = columns[count - 1 : count, 0:4]
    weight = step_column * jnp.exp(last - running)
    weighted = (x * spread(weight, HEAD_DIM)).astype(BF16)
    end_state = dot(weighted, b, (0, 0)).astype(BF16)
    high = last.astype(BF16).astype(F32)
    low = last - high
    half = iota((PIECE, lanes), 1) < lanes // 2
    for e in range(experts):
        head = e * PIECE // HEAD_DIM
        mine = routed[e * capacity : (e + 1) * capacity, :]
        send[e, 0:capacity, :] = mine[:, 0:lanes]
        send[e, capacity : 2 * capacity, :] = mine[:, lanes:]
        send[e, rows - 2 * PIECE : rows - PIECE, :] = end_state[e * PIECE : (e + 1) * PIECE]
        send[e, rows - PIECE :, :] = jnp.where(
            half, high[:, head : head + 1], low[:, head : head + 1]
        ).astype(BF16)


def enter_body(got, enter):
    sources, rows, lanes = got.shape
    size = sources * PIECE
    piece = got[:, rows - 2 * PIECE : rows - PIECE, :].reshape(size, lanes)
    logs = got[:, rows - PIECE :, :].reshape(size, lanes).astype(F32)
    logs = logs[:, 0:1] + logs[:, lanes // 2 : lanes // 2 + 1]
    row, column = iota((size, size), 0), iota((size, size), 1)
    before = column // PIECE < row // PIECE
    mean = jnp.where(before, 1.0 / PIECE, 0.0).astype(BF16)
    wide = jnp.broadcast_to(logs, (size, lanes))
    high = wide.astype(BF16)
    mid = (wide - high.astype(F32)).astype(BF16)
    low = (wide - high.astype(F32) - mid.astype(F32)).astype(BF16)
    earlier = dot(mean, high) + dot(mean, mid) + dot(mean, low)
    through = (earlier + wide).T[0:1, :]
    keep = before & (column % PIECE == row % PIECE)
    gap = jnp.where(keep, earlier[:, 0:1] - through, 0.0)
    decay = jnp.where(keep, jnp.exp(gap), 0.0)
    decay_high = decay.astype(BF16)
    decay_low = (decay - decay_high.astype(F32)).astype(BF16)
    result = dot(decay_high, piece) + dot(decay_low, piece)
    enter[...] = result.astype(BF16).reshape(sources, PIECE, lanes)


def inside_body(x_ref, b_ref, c_ref, columns, rows, bypass, out):
    count = x_ref.shape[0]
    scores = dot(c_ref[...], b_ref[...], (1, 1))
    causal = iota((count, count), 0) >= iota((count, count), 1)
    for head in range(4):
        part = slice(head * HEAD_DIM, (head + 1) * HEAD_DIM)
        gap = columns[:, head : head + 1] - rows[head : head + 1, :]
        weights = jnp.where(causal, jnp.exp(jnp.where(causal, gap, 0.0)), 0.0)
        x = x_ref[:, part]
        scaled = (x * columns[:, 4 + head : 5 + head]).astype(BF16)
        inside = dot((scores * weights).astype(BF16), scaled)
        out[:, part] = inside + bypass[head] * x


def finish_body(place, y, c, columns, enter, valve, gain, mine, other, normed):
    carried = dot(c[...], enter[...], (1, 1))
    carried = carried * spread(jnp.exp(columns[:, 0:4]), HEAD_DIM)
    gated = (y[...] + carried) * silu(valve[...].astype(F32))
    scale = lax.rsqrt(jnp.mean(gated * gated, axis=1, keepdims=True) + NORM_EPS)
    normed[...] = gated * scale * jnp.concatenate([gain[0:1, :], gain[1:2, :]], axis=1)
    chips = len(HOMES)
    rows = mine.shape[0] // chips
    for target, core in ((mine, place[0]), (other, 1 - place[0])):
        parts = []
        for k in HOMES:
            at = (2 * ((place[1] + k) % chips) + core) * rows
            parts.append(normed[pl.ds(pl.multiple_of(at, rows), rows), :])
        target[...] = jnp.concatenate(parts, axis=0).astype(BF16)


def joined_rows(piece, at, capacity):
    left = piece[at, 0:capacity, :]
    right = piece[at, capacity : 2 * capacity, :]
    rows, lanes = left.shape[0] * capacity, left.shape[2]
    return jnp.concatenate([left.reshape(rows, lanes), right.reshape(rows, lanes)], axis=1)


SOURCE_BLOCK = 8


def feature_sums(pieces, at, capacity, rows_of, gates, ups):
    gate = up = None
    for shift, piece in zip((0, 3, 1, 2), pieces):
        x = joined_rows(piece, at, capacity)
        rows = rows_of(shift)
        more = dot(x, gates[rows[0], :]), dot(x, ups[rows[1], :])
        gate, up = more if gate is None else (gate + more[0], up + more[1])
    return gate, up


def theirs_body(place, own, left, right, across, weights, out):
    sources, capacity = own.shape[0], own.shape[1] // 2
    size = 2 * own.shape[2]
    count = SOURCE_BLOCK * capacity

    def rows_of(shift):
        first = (place[1] + shift) % 4 * size
        return [pl.ds(pl.multiple_of(first + 4 * size * k, size), size) for k in range(2)]

    def step(i, _):
        at = pl.ds(i * SOURCE_BLOCK, SOURCE_BLOCK)
        to = pl.ds(pl.multiple_of(i * count, count), count)
        gate, up = feature_sums(
            (own, left, right, across), at, capacity, rows_of, weights, weights
        )
        width = gate.shape[1]
        out[to, 0:width] = gate.astype(BF16)
        out[to, width:] = up.astype(BF16)
        return 0

    lax.fori_loop(0, sources // SOURCE_BLOCK, step, 0)


def ours_body(place, own, left, right, across, valve, expand, other, rows, out):
    sources, capacity = own.shape[0], own.shape[1] // 2
    size = 2 * own.shape[2]
    count = SOURCE_BLOCK * capacity

    def rows_of(shift):
        first = place[0] * (4 * size) + (place[1] + shift) % 4 * size
        return [pl.ds(pl.multiple_of(first, size), size)] * 2

    def step(i, _):
        at = pl.ds(i * SOURCE_BLOCK, SOURCE_BLOCK)
        to = pl.ds(pl.multiple_of(i * count, count), count)
        gate, up = feature_sums((own, left, right, across), at, capacity, rows_of, valve, expand)
        width = gate.shape[1]
        gate = gate + other[to, 0:width].astype(F32)
        up = up + other[to, width:].astype(F32)
        out[to, :] = (silu(gate) * up).astype(BF16)
        return 0

    lax.fori_loop(0, sources // SOURCE_BLOCK, step, 0)
    out[sources * capacity :, :] = rows[...]


def split_body(place, valve, expand, contract, keep, give):
    half = valve.shape[0] // 2
    theirs = pl.ds(pl.multiple_of((1 - place[0]) * half, half), half)
    give[0:half, :] = valve[theirs, :]
    give[half : 2 * half, :] = expand[theirs, :]
    depth = contract.shape[0]
    for k, home in enumerate(HOMES):
        base = 2 * ((place[1] + home) % len(HOMES))
        row, lane = k // 2 * depth, k % 2 * 128
        for target, core, first in ((keep, place[0], 0), (give, 1 - place[0], 2 * half)):
            target[first + row : first + row + depth, lane : lane + 128] = contract[
                :, pl.ds(pl.multiple_of((base + core) * 128, 128), 128)
            ]


def down_body(start, own, far, rows, keep, weights, result, result_far, *outs):
    depth = own.shape[1]
    each = rows.shape[0] // len(HOMES)
    total = own.shape[0] - rows.shape[0]
    far_first = weights.shape[0] - keep.shape[0]
    block = total // 2

    def step(i, _):
        at = pl.ds(pl.multiple_of(i * block, block), block)
        near, beyond = own[at, :], far[at, :]
        for k in range(0, len(outs), 2):
            row = (start + k) // 2 * depth
            product = dot(near, keep[row : row + depth, :]) + dot(
                beyond, weights[far_first + row : far_first + row + depth, :]
            )
            for j in range(2):
                outs[k + j][at, :] = product[:, j * 128 : (j + 1) * 128].astype(BF16)
        return 0

    lax.fori_loop(0, total // block, step, 0)
    first, last = start * each, (start + len(outs)) * each
    near, beyond = rows[first:last, :], far[total + first : total + last, :]
    wide = 512
    for column in range(0, result.shape[1], wide):
        columns = slice(column, column + wide)
        product = dot(near, result[:, columns]) + dot(beyond, result_far[:, columns])
        product = product.astype(BF16)
        for k, out in enumerate(outs):
            for j in range(wide // 128):
                to = total + (column // 128 + j) * each
                out[to : to + each, :] = product[
                    k * each : (k + 1) * each, j * 128 : (j + 1) * 128
                ]


def rim_body(x, b, c, out, done):
    first, copies = 0, []
    for k, part in enumerate((x, b, c)):
        size = part.shape[1]
        copy = pltpu.make_async_copy(
            part.at[pl.ds(part.shape[0] - RIM, RIM), :],
            out.at[:, pl.ds(first, size)],
            done.at[k],
        )
        copy.start()
        copies.append(copy)
        first += size
    for copy in copies:
        copy.wait()


def last_rows(*parts):
    width = sum(part.shape[1] for part in parts)
    return pl.pallas_call(
        rim_body,
        out_shape=shaped(RIM, width),
        in_specs=[pl.BlockSpec(memory_space=pltpu.HBM)] * len(parts),
        out_specs=VMEM,
        scratch_shapes=[pltpu.SemaphoreType.DMA((len(parts),))],
    )(*parts)


def merge_body(place, stay_up, stay_down, from_left, from_right, from_across, up, down):
    far = from_across[...].astype(F32)
    core = jnp.full((1, 1), place[0])
    total = stay_up[...].astype(F32) + from_left[...].astype(F32)
    up[...] = (total + jnp.where(core == 0, far, 0.0)).astype(BF16)
    total = stay_down[...].astype(F32) + from_right[...].astype(F32)
    down[...] = (total + jnp.where(core == 1, far, 0.0)).astype(BF16)


def total_body(stay, left, right, up, down, out, rows_out):
    total = stay[...].astype(F32) + left[...].astype(F32) + right[...].astype(F32)
    total = (total + up[...].astype(F32) + down[...].astype(F32)).astype(BF16)
    count, lanes = out.shape
    rows, width = rows_out.shape
    out[...] = total[0:count]
    for j in range(width // lanes):
        first = count + j * rows
        rows_out[:, j * lanes : (j + 1) * lanes] = total[first : first + rows]


def combine_body(got, slots, coefs, out):
    sources, capacity, lanes = got.shape
    rows = got[...].reshape(sources * capacity, lanes)
    slot_ids = iota((rows.shape[0], slots.shape[1]), 0)
    padded = jnp.concatenate([coefs[...]] * (8 // TOPK), axis=0)
    columns = padded.T
    total = None
    for k in range(TOPK):
        chosen = (slot_ids == slots[k : k + 1, :]).astype(F32).astype(BF16)
        term = dot(chosen, rows, (0, 0)) * columns[:, k : k + 1]
        total = term if total is None else total + term
    out[...] = total.astype(BF16)


def local(
    blender_incoming_features,
    entry_latent_matrix,
    exit_latent_matrix,
    unactivated_valve,
    presoftplus_strides,
    extra_attenuation,
    incoming_feature_kernel,
    entry_latent_kernel,
    exit_latent_kernel,
    stride_offset_vector,
    attenuation_speed_exponent,
    bypass_coef_vector,
    cluster_rescale_coefs,
    blender_result_matrix,
    latter_microbatch_activations,
    specialist_rescale_coefs,
    specialist_valve_matrix,
    specialist_expand_matrix,
    specialist_contract_matrix,
    specialist_picks,
    selected_specialist_coefs,
):
    ep_count, chips = lax.axis_size(EP), lax.axis_size("tp_0")
    chip, core = lax.axis_index("tp_0"), lax.axis_index("tp_1")
    count, width = blender_incoming_features.shape
    state = entry_latent_matrix.shape[1]
    token_count, model_width = latter_microbatch_activations.shape
    capacity = 3 * token_count * TOPK // (2 * ep_count)
    lanes = model_width // lax.axis_size(TP)
    total_rows = ep_count * capacity
    place = (core.reshape(1), chip.reshape(1))
    valve = specialist_valve_matrix.reshape(model_width, -1)
    expand = specialist_expand_matrix.reshape(model_width, -1)
    contract = specialist_contract_matrix.reshape(-1, model_width)
    hidden_width = valve.shape[1]

    def permuted(x, axis, pairs):
        return lax.ppermute(x, axis, pairs)

    def around(x, distance):
        return permuted(x, "tp_0", [(i, (i + distance) % chips) for i in range(chips)])

    def across(x):
        pairs = []
        for i in range(chips):
            pairs.append((2 * i, 2 * ((i + 2) % chips)))
            pairs.append((2 * i + 1, 2 * ((i - 2) % chips) + 1))
        return permuted(x, TP, pairs)

    def partner(x):
        return permuted(x, "tp_1", [(0, 1), (1, 0)])

    def exchanged(x, axis):
        return lax.all_to_all(x, axis, 0, 0, tiled=True)

    rim = last_rows(blender_incoming_features, entry_latent_matrix, exit_latent_matrix)
    rim = permuted(rim, EP, [(i, i + 1) for i in range(ep_count - 1)])
    routed, slots = call(
        functools.partial(route_body, ep_count),
        (shaped(total_rows, 2 * lanes), shaped(TOPK, token_count, dtype=jnp.int32)),
        (
            (core * (chips // 2) + chip % (chips // 2)).reshape(1),
            latter_microbatch_activations,
            specialist_rescale_coefs,
            specialist_picks.T,
        ),
        1 << 30,
        None,
        smem=1,
    )
    send, x, b, c, columns, rows = call(
        filter_body,
        (
            shaped(ep_count, 2 * capacity + 2 * PIECE, lanes),
            shaped(count, width, dtype=F32),
            shaped(count, state),
            shaped(count, state),
            shaped(count, 8, dtype=F32),
            shaped(8, count, dtype=F32),
        ),
        (
            stride_offset_vector,
            attenuation_speed_exponent,
            routed,
            blender_incoming_features,
            entry_latent_matrix,
            exit_latent_matrix,
            rim,
            incoming_feature_kernel,
            entry_latent_kernel,
            exit_latent_kernel,
            presoftplus_strides.T,
            extra_attenuation.T,
        ),
        1 << 30,
        None,
        scratch=(pltpu.VMEM((RIM + count, width + 2 * state), F32),),
        smem=2,
    )
    got = exchanged(send, EP)
    y = inside(bypass_coef_vector, x, b, c, columns, rows)

    half = model_width // 2
    keep, give = call(
        placed(split_body),
        (shaped(half, hidden_width), shaped(3 * half, hidden_width)),
        (*place, valve, expand, contract),
        1 << 30,
        None,
        smem=2,
    )
    weights_far = partner(give)
    result_far = partner(blender_result_matrix)

    own = got[:, 0 : 2 * capacity, :]
    beyond = across(own)
    left, right = around(own, 1), around(own, -1)
    pieces = (own, left, right, beyond)
    theirs = call(
        placed(theirs_body),
        shaped(total_rows, 2 * hidden_width),
        (*place, *pieces, weights_far),
        1 << 31,
        10,
        smem=2,
    )
    theirs = partner(theirs)

    enter = call(enter_body, shaped(ep_count, PIECE, lanes), (got,), 1 << 30, 8)
    enter = exchanged(enter, EP).reshape(width, state)
    row_count = count // 2
    mine_rows, other_rows = call(
        placed(finish_body),
        (shaped(row_count, width),) * 2,
        (
            *place,
            y,
            c,
            columns,
            enter,
            unactivated_valve,
            cluster_rescale_coefs.astype(F32).reshape(-1, 128),
        ),
        1 << 31,
        8,
        scratch=(pltpu.VMEM((count, width), F32),),
        smem=2,
    )
    ours = call(
        placed(ours_body),
        shaped(total_rows + row_count, hidden_width),
        (*place, *pieces, valve, expand, theirs, other_rows),
        1 << 31,
        10,
        smem=2,
    )
    ours_far = partner(ours)
    row_block = count * model_width // (2 * chips * lanes)
    all_rows = total_rows + row_block

    def partials(start):
        return call(
            functools.partial(down_body, start),
            (shaped(all_rows, lanes),) * 4,
            (ours, ours_far, mine_rows, keep, weights_far, blender_result_matrix, result_far),
            1 << 31,
            12,
        )

    for_three, for_five, for_four, for_six = partials(0)
    from_across = across(for_four)
    from_left = around(for_three, 1)
    from_right = around(for_five, -1)
    for_one, for_seven, stay, for_two = partials(4)
    left_of_me, right_of_me = around(for_one, 1), around(for_seven, -1)
    up_two, down_two = call(
        placed(merge_body),
        (shaped(all_rows, lanes),) * 2,
        (*place, for_two, for_six, from_left, from_right, from_across),
        1 << 29,
        6,
        smem=2,
    )
    from_up, from_down = around(up_two, 2), around(down_two, -2)
    summed, mixed_a = call(
        total_body,
        (shaped(total_rows, lanes), shaped(count // (2 * chips), model_width)),
        (stay, left_of_me, right_of_me, from_up, from_down),
        1 << 29,
        4,
    )
    returned = exchanged(summed.reshape(ep_count, capacity, lanes), EP)
    mixed_b = call(
        combine_body,
        shaped(token_count, lanes),
        (returned, slots, selected_specialist_coefs.T),
        1 << 28,
        8,
    )
    return (mixed_a, mixed_b)


def inside(bypass, x, b, c, columns, rows):
    def body(bypass, x, b, c, columns, rows, out):
        inside_body(x, b, c, columns, rows, bypass, out)

    return call(
        body,
        shaped(*x.shape, dtype=F32),
        (bypass, x, b, c, columns, rows),
        1 << 31,
        None,
        smem=1,
    )


def solution(mesh):
    split = Mesh(mesh.devices.reshape(8, 4, 8, 2), ("ep_0", "ep_1", "tp_0", "tp_1"))
    in_specs = (
        P(EP, TP),
        P(EP, TP),
        P(EP, TP),
        P(EP, TP),
        P(EP, TP),
        P(EP, TP),
        P(None, TP),
        P(None, TP),
        P(None, TP),
        P(TP),
        P(TP),
        P(TP),
        P(TP),
        P(TP, None),
        P(EP, None),
        P(),
        P(EP, None, TP),
        P(EP, None, TP),
        P(EP, TP, None),
        P(EP, None),
        P(EP, None),
    )
    out_specs = (P(EP_TP, None), P(EP, TP))

    return jax.shard_map(local, mesh=split, in_specs=in_specs, out_specs=out_specs, check_vma=False)
```

```python
import functools

import jax
import jax.numpy as jnp
from jax import lax
from jax.experimental import pallas as pl
from jax.experimental.pallas import tpu as pltpu
from jax.sharding import Mesh
from jax.sharding import PartitionSpec as P


HEAD_DIM = 64
TOPK = 2
EP = ("ep_0", "ep_1")
TP = ("tp_0", "tp_1")
EP_TP = ("ep_0", "ep_1", "tp_0", "tp_1")
RIM = 8
PIECE = 8
HOMES = (3, 5, 4, 6, 1, 7, 0, 2)

NORM_EPS = 1e-06
F32 = jnp.float32
BF16 = jnp.bfloat16
VMEM = pl.BlockSpec(memory_space=pltpu.VMEM)
SMEM = pl.BlockSpec(memory_space=pltpu.SMEM)


def call(body, outs, ins, flops, room, scratch=(), smem=0, still=0):
    return pl.pallas_call(
        body,
        out_shape=outs,
        in_specs=[SMEM] * smem
        + [pl.BlockSpec(memory_space=pl.ANY)] * still
        + [VMEM] * (len(ins) - smem - still),
        out_specs=jax.tree.map(lambda _: VMEM, outs),
        scratch_shapes=scratch,
        cost_estimate=pl.CostEstimate(flops=flops, bytes_accessed=1 << 20, transcendentals=0),
        compiler_params=pltpu.CompilerParams(vmem_limit_bytes=room << 20 if room else None),
    )(*ins)


def placed(body):
    def run(core, chip, *refs):
        body((core[0], chip[0]), *refs)

    return run


def shaped(*shape, dtype=BF16):
    return jax.ShapeDtypeStruct(shape, dtype)


def iota(shape, dim):
    return lax.broadcasted_iota(jnp.int32, shape, dim)


def silu(v):
    return v * jax.nn.sigmoid(v)


def dot(a, b, contract=(1, 0)):
    return lax.dot_general(
        a, b, (((contract[0],), (contract[1],)), ((), ())), preferred_element_type=F32
    )


def spread(columns, width):
    lane_head = iota((columns.shape[0], 4 * width), 1) // width
    wide = columns[:, 0:1]
    for head in range(1, 4):
        wide = jnp.where(lane_head == head, columns[:, head : head + 1], wide)
    return wide


def route_body(
    experts,
    place,
    offset,
    speed,
    tokens,
    token_gain,
    picks,
    x_in,
    b_in,
    c_in,
    x_taps,
    b_taps,
    c_taps,
    strides,
    extra,
    routed,
    slots_out,
    x_out,
    b_out,
    c_out,
    heads_out,
    columns_out,
    rows_out,
    joined,
):
    lanes = 128
    total_rows, token_count = routed.shape[0], tokens.shape[0]
    capacity = total_rows // experts
    data = tokens[...].astype(F32)
    scale = lax.rsqrt(jnp.mean(data * data, axis=1, keepdims=True) + NORM_EPS)
    first = pl.multiple_of(place[0] * (2 * lanes), 2 * lanes)
    chosen = tokens[:, pl.ds(first, 2 * lanes)].astype(F32)
    gain = token_gain[pl.ds(first, 2 * lanes)].astype(F32).reshape(1, 2 * lanes)
    chosen = (chosen * scale * gain).astype(BF16)
    expert = iota((experts, token_count), 0)
    earlier = (
        iota((token_count, token_count), 0) < iota((token_count, token_count), 1)
    ).astype(BF16)
    base = jnp.zeros((experts, 1), F32)
    slot_ids = iota((total_rows, token_count), 0)
    placing = None
    for k in range(TOPK):
        pick = picks[k : k + 1, :]
        named = (expert == pick).astype(F32)
        rank = base + dot(named.astype(BF16), earlier)
        rank = jnp.sum(named * rank, axis=0, keepdims=True)
        slot = pick * capacity + rank.astype(jnp.int32)
        slots_out[k : k + 1, :] = slot
        base = base + jnp.sum(named, axis=1, keepdims=True)
        hit = slot_ids == slot
        placing = hit if placing is None else placing | hit
    routed[...] = dot(placing.astype(F32).astype(BF16), chosen).astype(BF16)

    count, width = x_in.shape
    state = b_in.shape[1]
    joined[0:RIM, :] = jnp.zeros((RIM, width + 2 * state), F32)
    joined[RIM:, 0:width] = x_in[...].astype(F32)
    joined[RIM:, width : width + state] = b_in[...].astype(F32)
    joined[RIM:, width + state :] = c_in[...].astype(F32)
    heads_out[...] = joined[RIM : 2 * RIM, :]
    x_out[...] = filtered(joined, count, 0, width, x_taps)
    b_out[...] = filtered(joined, count, width, state, b_taps).astype(BF16)
    c_out[...] = filtered(joined, count, width + state, state, c_taps).astype(BF16)

    def per_head(values):
        head = iota(strides.shape, 0)
        wide = jnp.full(strides.shape, values[0], F32)
        for k in range(1, strides.shape[0]):
            wide = jnp.where(head == k, values[k], wide)
        return wide

    raw = strides[...] + per_head(offset)
    step = jnp.maximum(raw, 0.0) + jnp.log1p(jnp.exp(-jnp.abs(raw)))
    total = -jnp.exp(per_head(speed)) * step + extra[...]
    both = jnp.concatenate([total, step], axis=0)
    lane = iota(both.shape, 1)
    shift = 1
    while shift < count:
        moved = jnp.where((lane >= shift), pltpu.roll(both, shift, axis=1), 0.0)
        both = jnp.where(iota(both.shape, 0) < 4, both + moved, both)
        shift *= 2
    columns_out[...] = both.T
    rows_out[...] = both


def filtered(joined, count, first, size, taps_ref):
    taps = taps_ref[...].astype(F32)
    total = None
    for j in range(taps.shape[0]):
        start = RIM - taps.shape[0] + 1 + j
        term = taps[j : j + 1] * joined[start : start + count, first : first + size]
        total = term if total is None else total + term
    return silu(total)


def filter_body(
    routed,
    x_in,
    b_in,
    c_in,
    heads,
    rim,
    x_taps,
    b_taps,
    c_taps,
    columns_in,
    send,
    x_out,
    b_out,
    c_out,
    joined,
):
    count, width = x_in.shape
    state = b_in.shape[1]
    experts, rows, lanes = send.shape
    capacity = (rows - 2 * PIECE) // 2
    joined[0:RIM, :] = rim[...].astype(F32)
    joined[RIM:, :] = heads[...]
    for source, target, first, size, taps in (
        (x_in, x_out, 0, width, x_taps),
        (b_in, b_out, width, state, b_taps),
        (c_in, c_out, width + state, state, c_taps),
    ):
        target[RIM:, :] = source[RIM:, :]
        target[0:RIM, :] = filtered(joined, RIM, first, size, taps).astype(target.dtype)
    columns = columns_in[...]
    running, step_column = columns[:, 0:4], columns[:, 4:8]
    last = columns[count - 1 : count, 0:4]
    weight = step_column * jnp.exp(last - running)
    weighted = (x_out[...] * spread(weight, HEAD_DIM)).astype(BF16)
    end_state = dot(weighted, b_out[...], (0, 0)).astype(BF16)
    high = last.astype(BF16).astype(F32)
    low = last - high
    half = iota((PIECE, lanes), 1) < lanes // 2
    for e in range(experts):
        head = e * PIECE // HEAD_DIM
        mine = routed[e * capacity : (e + 1) * capacity, :]
        send[e, 0:capacity, :] = mine[:, 0:lanes]
        send[e, capacity : 2 * capacity, :] = mine[:, lanes:]
        send[e, rows - 2 * PIECE : rows - PIECE, :] = end_state[e * PIECE : (e + 1) * PIECE]
        send[e, rows - PIECE :, :] = jnp.where(
            half, high[:, head : head + 1], low[:, head : head + 1]
        ).astype(BF16)


def enter_body(got, enter):
    sources, rows, lanes = got.shape
    size = sources * PIECE
    piece = got[:, rows - 2 * PIECE : rows - PIECE, :].reshape(size, lanes)
    logs = got[:, rows - PIECE :, :].reshape(size, lanes).astype(F32)
    logs = logs[:, 0:1] + logs[:, lanes // 2 : lanes // 2 + 1]
    row, column = iota((size, size), 0), iota((size, size), 1)
    before = column // PIECE < row // PIECE
    mean = jnp.where(before, 1.0 / PIECE, 0.0).astype(BF16)
    wide = jnp.broadcast_to(logs, (size, lanes))
    high = wide.astype(BF16)
    mid = (wide - high.astype(F32)).astype(BF16)
    low = (wide - high.astype(F32) - mid.astype(F32)).astype(BF16)
    earlier = dot(mean, high) + dot(mean, mid) + dot(mean, low)
    through = (earlier + wide).T[0:1, :]
    keep = before & (column % PIECE == row % PIECE)
    gap = jnp.where(keep, earlier[:, 0:1] - through, 0.0)
    decay = jnp.where(keep, jnp.exp(gap), 0.0)
    decay_high = decay.astype(BF16)
    decay_low = (decay - decay_high.astype(F32)).astype(BF16)
    result = dot(decay_high, piece) + dot(decay_low, piece)
    enter[...] = result.astype(BF16).reshape(sources, PIECE, lanes)


def inside_body(x_ref, b_ref, c_ref, columns, rows, bypass, out):
    count = x_ref.shape[0]
    scores = dot(c_ref[...], b_ref[...], (1, 1))
    causal = iota((count, count), 0) >= iota((count, count), 1)
    for head in range(4):
        part = slice(head * HEAD_DIM, (head + 1) * HEAD_DIM)
        gap = columns[:, head : head + 1] - rows[head : head + 1, :]
        weights = jnp.where(causal, jnp.exp(jnp.where(causal, gap, 0.0)), 0.0)
        x = x_ref[:, part]
        scaled = (x * columns[:, 4 + head : 5 + head]).astype(BF16)
        inside = dot((scores * weights).astype(BF16), scaled)
        out[:, part] = inside + bypass[head] * x


def finish_body(place, y, c, columns, enter, valve, gain, mine, other, normed):
    carried = dot(c[...], enter[...], (1, 1))
    carried = carried * spread(jnp.exp(columns[:, 0:4]), HEAD_DIM)
    gated = (y[...] + carried) * silu(valve[...].astype(F32))
    scale = lax.rsqrt(jnp.mean(gated * gated, axis=1, keepdims=True) + NORM_EPS)
    normed[...] = gated * scale * jnp.concatenate([gain[0:1, :], gain[1:2, :]], axis=1)
    chips = len(HOMES)
    rows = mine.shape[0] // chips
    for target, core in ((mine, place[0]), (other, 1 - place[0])):
        parts = []
        for k in HOMES:
            at = (2 * ((place[1] + k) % chips) + core) * rows
            parts.append(normed[pl.ds(pl.multiple_of(at, rows), rows), :])
        target[...] = jnp.concatenate(parts, axis=0).astype(BF16)


def joined_rows(piece, at, capacity):
    left = piece[at, 0:capacity, :]
    right = piece[at, capacity : 2 * capacity, :]
    rows, lanes = left.shape[0] * capacity, left.shape[2]
    return jnp.concatenate([left.reshape(rows, lanes), right.reshape(rows, lanes)], axis=1)


SOURCE_BLOCK = 8


def feature_sums(pieces, at, capacity, rows_of, gates, ups):
    gate = up = None
    for shift, piece in zip((0, 3, 1, 2), pieces):
        x = joined_rows(piece, at, capacity)
        rows = rows_of(shift)
        more = dot(x, gates[rows[0], :]), dot(x, ups[rows[1], :])
        gate, up = more if gate is None else (gate + more[0], up + more[1])
    return gate, up


def theirs_body(place, own, left, right, across, weights, out):
    sources, capacity = own.shape[0], own.shape[1] // 2
    size = 2 * own.shape[2]
    count = SOURCE_BLOCK * capacity

    def rows_of(shift):
        first = (place[1] + shift) % 4 * size
        return [pl.ds(pl.multiple_of(first + 4 * size * k, size), size) for k in range(2)]

    def step(i, _):
        at = pl.ds(i * SOURCE_BLOCK, SOURCE_BLOCK)
        to = pl.ds(pl.multiple_of(i * count, count), count)
        gate, up = feature_sums(
            (own, left, right, across), at, capacity, rows_of, weights, weights
        )
        width = gate.shape[1]
        out[to, 0:width] = gate.astype(BF16)
        out[to, width:] = up.astype(BF16)
        return 0

    lax.fori_loop(0, sources // SOURCE_BLOCK, step, 0)


def ours_body(place, own, left, right, across, valve, expand, other, rows, out):
    sources, capacity = own.shape[0], own.shape[1] // 2
    size = 2 * own.shape[2]
    count = SOURCE_BLOCK * capacity

    def rows_of(shift):
        first = place[0] * (4 * size) + (place[1] + shift) % 4 * size
        return [pl.ds(pl.multiple_of(first, size), size)] * 2

    def step(i, _):
        at = pl.ds(i * SOURCE_BLOCK, SOURCE_BLOCK)
        to = pl.ds(pl.multiple_of(i * count, count), count)
        gate, up = feature_sums((own, left, right, across), at, capacity, rows_of, valve, expand)
        width = gate.shape[1]
        gate = gate + other[to, 0:width].astype(F32)
        up = up + other[to, width:].astype(F32)
        out[to, :] = (silu(gate) * up).astype(BF16)
        return 0

    lax.fori_loop(0, sources // SOURCE_BLOCK, step, 0)
    out[sources * capacity :, :] = rows[...]


def split_body(place, valve, expand, contract, keep, give):
    half = valve.shape[0] // 2
    theirs = pl.ds(pl.multiple_of((1 - place[0]) * half, half), half)
    give[0:half, :] = valve[theirs, :]
    give[half : 2 * half, :] = expand[theirs, :]
    depth = contract.shape[0]
    for k, home in enumerate(HOMES):
        base = 2 * ((place[1] + home) % len(HOMES))
        row, lane = k // 2 * depth, k % 2 * 128
        for target, core, first in ((keep, place[0], 0), (give, 1 - place[0], 2 * half)):
            target[first + row : first + row + depth, lane : lane + 128] = contract[
                :, pl.ds(pl.multiple_of((base + core) * 128, 128), 128)
            ]


def project_body(rows, result, out):
    wide = 512
    for column in range(0, result.shape[1], wide):
        columns = slice(column, column + wide)
        out[:, columns] = dot(rows[...], result[:, columns])


def down_body(start, own, far, rows, keep, weights, result_far, *outs):
    depth = own.shape[1]
    each = rows.shape[0] // len(HOMES)
    total = own.shape[0] - rows.shape[0]
    far_first = weights.shape[0] - keep.shape[0]
    block = total // 2

    def step(i, _):
        at = pl.ds(pl.multiple_of(i * block, block), block)
        near, beyond = own[at, :], far[at, :]
        for k in range(0, len(outs), 2):
            row = (start + k) // 2 * depth
            product = dot(near, keep[row : row + depth, :]) + dot(
                beyond, weights[far_first + row : far_first + row + depth, :]
            )
            for j in range(2):
                outs[k + j][at, :] = product[:, j * 128 : (j + 1) * 128].astype(BF16)
        return 0

    lax.fori_loop(0, total // block, step, 0)
    first, last = start * each, (start + len(outs)) * each
    beyond = far[total + first : total + last, :]
    wide = 512
    for column in range(0, rows.shape[1], wide):
        columns = slice(column, column + wide)
        product = rows[first:last, columns] + dot(beyond, result_far[:, columns])
        product = product.astype(BF16)
        for k, out in enumerate(outs):
            for j in range(wide // 128):
                to = total + (column // 128 + j) * each
                out[to : to + each, :] = product[
                    k * each : (k + 1) * each, j * 128 : (j + 1) * 128
                ]


def rim_body(x, b, c, out, done):
    first, copies = 0, []
    for k, part in enumerate((x, b, c)):
        size = part.shape[1]
        copy = pltpu.make_async_copy(
            part.at[pl.ds(part.shape[0] - RIM, RIM), :],
            out.at[:, pl.ds(first, size)],
            done.at[k],
        )
        copy.start()
        copies.append(copy)
        first += size
    for copy in copies:
        copy.wait()


def last_rows(*parts):
    width = sum(part.shape[1] for part in parts)
    return pl.pallas_call(
        rim_body,
        out_shape=shaped(RIM, width),
        in_specs=[pl.BlockSpec(memory_space=pltpu.HBM)] * len(parts),
        out_specs=VMEM,
        scratch_shapes=[pltpu.SemaphoreType.DMA((len(parts),))],
    )(*parts)


def merge_body(place, stay_up, stay_down, from_left, from_right, from_across, up, down):
    far = from_across[...].astype(F32)
    core = jnp.full((1, 1), place[0])
    total = stay_up[...].astype(F32) + from_left[...].astype(F32)
    up[...] = (total + jnp.where(core == 0, far, 0.0)).astype(BF16)
    total = stay_down[...].astype(F32) + from_right[...].astype(F32)
    down[...] = (total + jnp.where(core == 1, far, 0.0)).astype(BF16)


def total_body(stay, left, right, up, down, out, rows_out):
    total = stay[...].astype(F32) + left[...].astype(F32) + right[...].astype(F32)
    total = (total + up[...].astype(F32) + down[...].astype(F32)).astype(BF16)
    count, lanes = out.shape
    rows, width = rows_out.shape
    out[...] = total[0:count]
    for j in range(width // lanes):
        first = count + j * rows
        rows_out[:, j * lanes : (j + 1) * lanes] = total[first : first + rows]


def combine_body(got, slots, coefs, out):
    sources, capacity, lanes = got.shape
    rows = got[...].reshape(sources * capacity, lanes)
    slot_ids = iota((rows.shape[0], slots.shape[1]), 0)
    padded = jnp.concatenate([coefs[...]] * (8 // TOPK), axis=0)
    columns = padded.T
    total = None
    for k in range(TOPK):
        chosen = (slot_ids == slots[k : k + 1, :]).astype(F32).astype(BF16)
        term = dot(chosen, rows, (0, 0)) * columns[:, k : k + 1]
        total = term if total is None else total + term
    out[...] = total.astype(BF16)


def local(
    blender_incoming_features,
    entry_latent_matrix,
    exit_latent_matrix,
    unactivated_valve,
    presoftplus_strides,
    extra_attenuation,
    incoming_feature_kernel,
    entry_latent_kernel,
    exit_latent_kernel,
    stride_offset_vector,
    attenuation_speed_exponent,
    bypass_coef_vector,
    cluster_rescale_coefs,
    blender_result_matrix,
    latter_microbatch_activations,
    specialist_rescale_coefs,
    specialist_valve_matrix,
    specialist_expand_matrix,
    specialist_contract_matrix,
    specialist_picks,
    selected_specialist_coefs,
):
    ep_count, chips = lax.axis_size(EP), lax.axis_size("tp_0")
    chip, core = lax.axis_index("tp_0"), lax.axis_index("tp_1")
    count, width = blender_incoming_features.shape
    state = entry_latent_matrix.shape[1]
    token_count, model_width = latter_microbatch_activations.shape
    capacity = 3 * token_count * TOPK // (2 * ep_count)
    lanes = model_width // lax.axis_size(TP)
    total_rows = ep_count * capacity
    place = (core.reshape(1), chip.reshape(1))
    valve = specialist_valve_matrix.reshape(model_width, -1)
    expand = specialist_expand_matrix.reshape(model_width, -1)
    contract = specialist_contract_matrix.reshape(-1, model_width)
    hidden_width = valve.shape[1]

    def permuted(x, axis, pairs):
        return lax.ppermute(x, axis, pairs)

    def around(x, distance):
        return permuted(x, "tp_0", [(i, (i + distance) % chips) for i in range(chips)])

    def across(x):
        pairs = []
        for i in range(chips):
            pairs.append((2 * i, 2 * ((i + 2) % chips)))
            pairs.append((2 * i + 1, 2 * ((i - 2) % chips) + 1))
        return permuted(x, TP, pairs)

    def partner(x):
        return permuted(x, "tp_1", [(0, 1), (1, 0)])

    def exchanged(x, axis):
        return lax.all_to_all(x, axis, 0, 0, tiled=True)

    rim = last_rows(blender_incoming_features, entry_latent_matrix, exit_latent_matrix)
    rim = permuted(rim, EP, [(i, i + 1) for i in range(ep_count - 1)])
    taps = (incoming_feature_kernel, entry_latent_kernel, exit_latent_kernel)
    filtered_shapes = (
        shaped(count, width, dtype=F32),
        shaped(count, state),
        shaped(count, state),
    )
    routed, slots, x, b, c, heads, columns, rows = call(
        functools.partial(route_body, ep_count),
        (
            shaped(total_rows, 2 * lanes),
            shaped(TOPK, token_count, dtype=jnp.int32),
            *filtered_shapes,
            shaped(RIM, width + 2 * state, dtype=F32),
            shaped(count, 8, dtype=F32),
            shaped(8, count, dtype=F32),
        ),
        (
            (core * (chips // 2) + chip % (chips // 2)).reshape(1),
            stride_offset_vector,
            attenuation_speed_exponent,
            latter_microbatch_activations,
            specialist_rescale_coefs,
            specialist_picks.T,
            blender_incoming_features,
            entry_latent_matrix,
            exit_latent_matrix,
            *taps,
            presoftplus_strides.T,
            extra_attenuation.T,
        ),
        1 << 30,
        None,
        scratch=(pltpu.VMEM((RIM + count, width + 2 * state), F32),),
        smem=3,
    )
    send, x, b, c = call(
        filter_body,
        (shaped(ep_count, 2 * capacity + 2 * PIECE, lanes), *filtered_shapes),
        (routed, x, b, c, heads, rim, *taps, columns),
        1 << 30,
        None,
        scratch=(pltpu.VMEM((2 * RIM, width + 2 * state), F32),),
    )
    got = exchanged(send, EP)
    y = inside(bypass_coef_vector, x, b, c, columns, rows)

    half = model_width // 2
    keep, give = call(
        placed(split_body),
        (shaped(half, hidden_width), shaped(3 * half, hidden_width)),
        (*place, valve, expand, contract),
        1 << 30,
        None,
        smem=2,
    )
    weights_far = partner(give)
    result_far = partner(blender_result_matrix)

    own = got[:, 0 : 2 * capacity, :]
    beyond = across(own)
    left, right = around(own, 1), around(own, -1)
    pieces = (own, left, right, beyond)
    theirs = call(
        placed(theirs_body),
        shaped(total_rows, 2 * hidden_width),
        (*place, *pieces, weights_far),
        1 << 31,
        10,
        smem=2,
    )
    theirs = partner(theirs)

    enter = call(enter_body, shaped(ep_count, PIECE, lanes), (got,), 1 << 30, 8)
    enter = exchanged(enter, EP).reshape(width, state)
    row_count = count // 2
    mine_rows, other_rows = call(
        placed(finish_body),
        (shaped(row_count, width),) * 2,
        (
            *place,
            y,
            c,
            columns,
            enter,
            unactivated_valve,
            cluster_rescale_coefs.astype(F32).reshape(-1, 128),
        ),
        1 << 31,
        8,
        scratch=(pltpu.VMEM((count, width), F32),),
        smem=2,
    )
    ours = call(
        placed(ours_body),
        shaped(total_rows + row_count, hidden_width),
        (*place, *pieces, valve, expand, theirs, other_rows),
        1 << 31,
        10,
        smem=2,
    )
    ours_far = partner(ours)
    row_block = count * model_width // (2 * chips * lanes)
    all_rows = total_rows + row_block
    projected = call(
        project_body,
        shaped(row_count, model_width, dtype=F32),
        (mine_rows, blender_result_matrix),
        1 << 29,
        6,
    )

    def partials(start):
        return call(
            functools.partial(down_body, start),
            (shaped(all_rows, lanes),) * 4,
            (ours, ours_far, projected, keep, weights_far, result_far),
            1 << 31,
            12,
        )

    for_three, for_five, for_four, for_six = partials(0)
    from_across = across(for_four)
    from_left = around(for_three, 1)
    from_right = around(for_five, -1)
    for_one, for_seven, stay, for_two = partials(4)
    left_of_me, right_of_me = around(for_one, 1), around(for_seven, -1)
    up_two, down_two = call(
        placed(merge_body),
        (shaped(all_rows, lanes),) * 2,
        (*place, for_two, for_six, from_left, from_right, from_across),
        1 << 29,
        6,
        smem=2,
    )
    from_up, from_down = around(up_two, 2), around(down_two, -2)
    summed, mixed_a = call(
        total_body,
        (shaped(total_rows, lanes), shaped(count // (2 * chips), model_width)),
        (stay, left_of_me, right_of_me, from_up, from_down),
        1 << 29,
        4,
    )
    returned = exchanged(summed.reshape(ep_count, capacity, lanes), EP)
    mixed_b = call(
        combine_body,
        shaped(token_count, lanes),
        (returned, slots, selected_specialist_coefs.T),
        1 << 28,
        8,
    )
    return (mixed_a, mixed_b)


def inside(bypass, x, b, c, columns, rows):
    def body(bypass, x, b, c, columns, rows, out):
        inside_body(x, b, c, columns, rows, bypass, out)

    return call(
        body,
        shaped(*x.shape, dtype=F32),
        (bypass, x, b, c, columns, rows),
        1 << 31,
        None,
        smem=1,
    )


def solution(mesh):
    split = Mesh(mesh.devices.reshape(8, 4, 8, 2), ("ep_0", "ep_1", "tp_0", "tp_1"))
    in_specs = (
        P(EP, TP),
        P(EP, TP),
        P(EP, TP),
        P(EP, TP),
        P(EP, TP),
        P(EP, TP),
        P(None, TP),
        P(None, TP),
        P(None, TP),
        P(TP),
        P(TP),
        P(TP),
        P(TP),
        P(TP, None),
        P(EP, None),
        P(),
        P(EP, None, TP),
        P(EP, None, TP),
        P(EP, TP, None),
        P(EP, None),
        P(EP, None),
    )
    out_specs = (P(EP_TP, None), P(EP, TP))

    return jax.shard_map(local, mesh=split, in_specs=in_specs, out_specs=out_specs, check_vma=False)
```

```python
import functools

import jax
import jax.numpy as jnp
from jax import lax
from jax.experimental import pallas as pl
from jax.experimental.pallas import tpu as pltpu
from jax.sharding import Mesh
from jax.sharding import PartitionSpec as P


HEAD_DIM = 64
TOPK = 2
EP = ("ep_0", "ep_1")
TP = ("tp_0", "tp_1")
EP_TP = ("ep_0", "ep_1", "tp_0", "tp_1")
RIM = 8
PIECE = 8
HOMES = (3, 5, 4, 6, 1, 7, 0, 2)

NORM_EPS = 1e-06
F32 = jnp.float32
BF16 = jnp.bfloat16
VMEM = pl.BlockSpec(memory_space=pltpu.VMEM)
SMEM = pl.BlockSpec(memory_space=pltpu.SMEM)


def call(body, outs, ins, flops, room, scratch=(), smem=0, still=0):
    return pl.pallas_call(
        body,
        out_shape=outs,
        in_specs=[SMEM] * smem
        + [pl.BlockSpec(memory_space=pl.ANY)] * still
        + [VMEM] * (len(ins) - smem - still),
        out_specs=jax.tree.map(lambda _: VMEM, outs),
        scratch_shapes=scratch,
        cost_estimate=pl.CostEstimate(flops=flops, bytes_accessed=1 << 20, transcendentals=0),
        compiler_params=pltpu.CompilerParams(vmem_limit_bytes=room << 20 if room else None),
    )(*ins)


def placed(body):
    def run(core, chip, *refs):
        body((core[0], chip[0]), *refs)

    return run


def shaped(*shape, dtype=BF16):
    return jax.ShapeDtypeStruct(shape, dtype)


def iota(shape, dim):
    return lax.broadcasted_iota(jnp.int32, shape, dim)


def silu(v):
    return v * jax.nn.sigmoid(v)


def dot(a, b, contract=(1, 0)):
    return lax.dot_general(
        a, b, (((contract[0],), (contract[1],)), ((), ())), preferred_element_type=F32
    )


def spread(columns, width):
    lane_head = iota((columns.shape[0], 4 * width), 1) // width
    wide = columns[:, 0:1]
    for head in range(1, 4):
        wide = jnp.where(lane_head == head, columns[:, head : head + 1], wide)
    return wide


def route_body(
    experts,
    place,
    offset,
    speed,
    tokens,
    token_gain,
    picks,
    x_in,
    b_in,
    c_in,
    x_taps,
    b_taps,
    c_taps,
    strides,
    extra,
    routed,
    slots_out,
    x_out,
    b_out,
    c_out,
    heads_out,
    columns_out,
    rows_out,
    joined,
):
    lanes = 128
    total_rows, token_count = routed.shape[0], tokens.shape[0]
    capacity = total_rows // experts
    data = tokens[...].astype(F32)
    scale = lax.rsqrt(jnp.mean(data * data, axis=1, keepdims=True) + NORM_EPS)
    first = pl.multiple_of(place[0] * (2 * lanes), 2 * lanes)
    chosen = tokens[:, pl.ds(first, 2 * lanes)].astype(F32)
    gain = token_gain[pl.ds(first, 2 * lanes)].astype(F32).reshape(1, 2 * lanes)
    chosen = (chosen * scale * gain).astype(BF16)
    expert = iota((experts, token_count), 0)
    earlier = (
        iota((token_count, token_count), 0) < iota((token_count, token_count), 1)
    ).astype(BF16)
    base = jnp.zeros((experts, 1), F32)
    slot_ids = iota((total_rows, token_count), 0)
    placing = None
    for k in range(TOPK):
        pick = picks[k : k + 1, :]
        named = (expert == pick).astype(F32)
        rank = base + dot(named.astype(BF16), earlier)
        rank = jnp.sum(named * rank, axis=0, keepdims=True)
        slot = pick * capacity + rank.astype(jnp.int32)
        slots_out[k : k + 1, :] = slot
        base = base + jnp.sum(named, axis=1, keepdims=True)
        hit = slot_ids == slot
        placing = hit if placing is None else placing | hit
    routed[...] = dot(placing.astype(F32).astype(BF16), chosen).astype(BF16)

    count, width = x_in.shape
    state = b_in.shape[1]
    joined[0:RIM, :] = jnp.zeros((RIM, width + 2 * state), F32)
    joined[RIM:, 0:width] = x_in[...].astype(F32)
    joined[RIM:, width : width + state] = b_in[...].astype(F32)
    joined[RIM:, width + state :] = c_in[...].astype(F32)
    heads_out[...] = joined[RIM : 2 * RIM, :]
    x_out[...] = filtered(joined, count, 0, width, x_taps)
    b_out[...] = filtered(joined, count, width, state, b_taps).astype(BF16)
    c_out[...] = filtered(joined, count, width + state, state, c_taps).astype(BF16)

    def per_head(values):
        head = iota(strides.shape, 0)
        wide = jnp.full(strides.shape, values[0], F32)
        for k in range(1, strides.shape[0]):
            wide = jnp.where(head == k, values[k], wide)
        return wide

    raw = strides[...] + per_head(offset)
    step = jnp.maximum(raw, 0.0) + jnp.log1p(jnp.exp(-jnp.abs(raw)))
    total = -jnp.exp(per_head(speed)) * step + extra[...]
    both = jnp.concatenate([total, step], axis=0)
    lane = iota(both.shape, 1)
    shift = 1
    while shift < count:
        moved = jnp.where((lane >= shift), pltpu.roll(both, shift, axis=1), 0.0)
        both = jnp.where(iota(both.shape, 0) < 4, both + moved, both)
        shift *= 2
    columns_out[...] = both.T
    rows_out[...] = both


def filtered(joined, count, first, size, taps_ref):
    taps = taps_ref[...].astype(F32)
    total = None
    for j in range(taps.shape[0]):
        start = RIM - taps.shape[0] + 1 + j
        term = taps[j : j + 1] * joined[start : start + count, first : first + size]
        total = term if total is None else total + term
    return silu(total)


def filter_body(
    routed,
    x_in,
    b_in,
    c_in,
    heads,
    rim,
    x_taps,
    b_taps,
    c_taps,
    columns_in,
    send,
    x_out,
    b_out,
    c_out,
    joined,
):
    count, width = x_in.shape
    state = b_in.shape[1]
    experts, rows, lanes = send.shape
    capacity = (rows - 2 * PIECE) // 2
    joined[0:RIM, :] = rim[...].astype(F32)
    joined[RIM:, :] = heads[...]
    for source, target, first, size, taps in (
        (x_in, x_out, 0, width, x_taps),
        (b_in, b_out, width, state, b_taps),
        (c_in, c_out, width + state, state, c_taps),
    ):
        target[RIM:, :] = source[RIM:, :]
        target[0:RIM, :] = filtered(joined, RIM, first, size, taps).astype(target.dtype)
    columns = columns_in[...]
    running, step_column = columns[:, 0:4], columns[:, 4:8]
    last = columns[count - 1 : count, 0:4]
    weight = step_column * jnp.exp(last - running)
    weighted = (x_out[...] * spread(weight, HEAD_DIM)).astype(BF16)
    end_state = dot(weighted, b_out[...], (0, 0)).astype(BF16)
    high = last.astype(BF16).astype(F32)
    low = last - high
    half = iota((PIECE, lanes), 1) < lanes // 2
    for e in range(experts):
        head = e * PIECE // HEAD_DIM
        mine = routed[e * capacity : (e + 1) * capacity, :]
        send[e, 0:capacity, :] = mine[:, 0:lanes]
        send[e, capacity : 2 * capacity, :] = mine[:, lanes:]
        send[e, rows - 2 * PIECE : rows - PIECE, :] = end_state[e * PIECE : (e + 1) * PIECE]
        send[e, rows - PIECE :, :] = jnp.where(
            half, high[:, head : head + 1], low[:, head : head + 1]
        ).astype(BF16)


def enter_body(got, enter):
    sources, rows, lanes = got.shape
    size = sources * PIECE
    piece = got[:, rows - 2 * PIECE : rows - PIECE, :].reshape(size, lanes)
    logs = got[:, rows - PIECE :, :].reshape(size, lanes).astype(F32)
    logs = logs[:, 0:1] + logs[:, lanes // 2 : lanes // 2 + 1]
    row, column = iota((size, size), 0), iota((size, size), 1)
    before = column // PIECE < row // PIECE
    mean = jnp.where(before, 1.0 / PIECE, 0.0).astype(BF16)
    wide = jnp.broadcast_to(logs, (size, lanes))
    high = wide.astype(BF16)
    mid = (wide - high.astype(F32)).astype(BF16)
    low = (wide - high.astype(F32) - mid.astype(F32)).astype(BF16)
    earlier = dot(mean, high) + dot(mean, mid) + dot(mean, low)
    through = (earlier + wide).T[0:1, :]
    keep = before & (column % PIECE == row % PIECE)
    gap = jnp.where(keep, earlier[:, 0:1] - through, 0.0)
    decay = jnp.where(keep, jnp.exp(gap), 0.0)
    decay_high = decay.astype(BF16)
    decay_low = (decay - decay_high.astype(F32)).astype(BF16)
    result = dot(decay_high, piece) + dot(decay_low, piece)
    enter[...] = result.astype(BF16).reshape(sources, PIECE, lanes)


def inside_body(x_ref, b_ref, c_ref, columns, rows, bypass, out):
    count = x_ref.shape[0]
    scores = dot(c_ref[...], b_ref[...], (1, 1))
    causal = iota((count, count), 0) >= iota((count, count), 1)
    for head in range(4):
        part = slice(head * HEAD_DIM, (head + 1) * HEAD_DIM)
        gap = columns[:, head : head + 1] - rows[head : head + 1, :]
        weights = jnp.where(causal, jnp.exp(jnp.where(causal, gap, 0.0)), 0.0)
        x = x_ref[:, part]
        scaled = (x * columns[:, 4 + head : 5 + head]).astype(BF16)
        inside = dot((scores * weights).astype(BF16), scaled)
        out[:, part] = inside + bypass[head] * x


def finish_body(place, y, c, columns, enter, valve, gain, mine, other, normed):
    carried = dot(c[...], enter[...], (1, 1))
    carried = carried * spread(jnp.exp(columns[:, 0:4]), HEAD_DIM)
    gated = (y[...] + carried) * silu(valve[...].astype(F32))
    scale = lax.rsqrt(jnp.mean(gated * gated, axis=1, keepdims=True) + NORM_EPS)
    normed[...] = gated * scale * jnp.concatenate([gain[0:1, :], gain[1:2, :]], axis=1)
    chips = len(HOMES)
    rows = mine.shape[0] // chips
    for target, core in ((mine, place[0]), (other, 1 - place[0])):
        parts = []
        for k in HOMES:
            at = (2 * ((place[1] + k) % chips) + core) * rows
            parts.append(normed[pl.ds(pl.multiple_of(at, rows), rows), :])
        target[...] = jnp.concatenate(parts, axis=0).astype(BF16)


def joined_rows(piece, at, capacity):
    left = piece[at, 0:capacity, :]
    right = piece[at, capacity : 2 * capacity, :]
    rows, lanes = left.shape[0] * capacity, left.shape[2]
    return jnp.concatenate([left.reshape(rows, lanes), right.reshape(rows, lanes)], axis=1)


SOURCE_BLOCK = 8


def feature_sums(pieces, at, capacity, rows_of, gates, ups):
    gate = up = None
    for shift, piece in zip((0, 3, 1, 2), pieces):
        x = joined_rows(piece, at, capacity)
        rows = rows_of(shift)
        more = dot(x, gates[rows[0], :]), dot(x, ups[rows[1], :])
        gate, up = more if gate is None else (gate + more[0], up + more[1])
    return gate, up


def theirs_body(place, own, left, right, across, weights, out):
    sources, capacity = own.shape[0], own.shape[1] // 2
    size = 2 * own.shape[2]
    count = SOURCE_BLOCK * capacity

    def rows_of(shift):
        first = (place[1] + shift) % 4 * size
        return [pl.ds(pl.multiple_of(first + 4 * size * k, size), size) for k in range(2)]

    def step(i, _):
        at = pl.ds(i * SOURCE_BLOCK, SOURCE_BLOCK)
        to = pl.ds(pl.multiple_of(i * count, count), count)
        gate, up = feature_sums(
            (own, left, right, across), at, capacity, rows_of, weights, weights
        )
        width = gate.shape[1]
        out[to, 0:width] = gate.astype(BF16)
        out[to, width:] = up.astype(BF16)
        return 0

    lax.fori_loop(0, sources // SOURCE_BLOCK, step, 0)


def ours_body(place, own, left, right, across, valve, expand, other, rows, out):
    sources, capacity = own.shape[0], own.shape[1] // 2
    size = 2 * own.shape[2]
    count = SOURCE_BLOCK * capacity

    def rows_of(shift):
        first = place[0] * (4 * size) + (place[1] + shift) % 4 * size
        return [pl.ds(pl.multiple_of(first, size), size)] * 2

    def step(i, _):
        at = pl.ds(i * SOURCE_BLOCK, SOURCE_BLOCK)
        to = pl.ds(pl.multiple_of(i * count, count), count)
        gate, up = feature_sums((own, left, right, across), at, capacity, rows_of, valve, expand)
        width = gate.shape[1]
        gate = gate + other[to, 0:width].astype(F32)
        up = up + other[to, width:].astype(F32)
        out[to, :] = (silu(gate) * up).astype(BF16)
        return 0

    lax.fori_loop(0, sources // SOURCE_BLOCK, step, 0)
    out[sources * capacity :, :] = rows[...]


def split_body(place, valve, expand, contract, result, keep, give):
    half, width = valve.shape[0] // 2, valve.shape[1]
    theirs = pl.ds(pl.multiple_of((1 - place[0]) * half, half), half)
    give[0:half, :] = valve[theirs, :]
    give[half : 2 * half, :] = expand[theirs, :]
    depth = contract.shape[0]
    for k in range(result.shape[1] // width):
        row = 3 * half + k * depth
        give[row : row + depth, :] = result[:, k * width : (k + 1) * width]
    for k, home in enumerate(HOMES):
        base = 2 * ((place[1] + home) % len(HOMES))
        row, lane = k // 2 * depth, k % 2 * 128
        for target, core, first in ((keep, place[0], 0), (give, 1 - place[0], 2 * half)):
            target[first + row : first + row + depth, lane : lane + 128] = contract[
                :, pl.ds(pl.multiple_of((base + core) * 128, 128), 128)
            ]


def project_body(rows, result, out):
    wide = 512
    for column in range(0, result.shape[1], wide):
        columns = slice(column, column + wide)
        out[:, columns] = dot(rows[...], result[:, columns])


def down_body(start, own, far, rows, keep, weights, *outs):
    depth = own.shape[1]
    each = rows.shape[0] // len(HOMES)
    total = own.shape[0] - rows.shape[0]
    far_first = 2 * keep.shape[0]
    block = total // 2

    def step(i, _):
        at = pl.ds(pl.multiple_of(i * block, block), block)
        near, beyond = own[at, :], far[at, :]
        for k in range(0, len(outs), 2):
            row = (start + k) // 2 * depth
            product = dot(near, keep[row : row + depth, :]) + dot(
                beyond, weights[far_first + row : far_first + row + depth, :]
            )
            for j in range(2):
                outs[k + j][at, :] = product[:, j * 128 : (j + 1) * 128].astype(BF16)
        return 0

    lax.fori_loop(0, total // block, step, 0)
    first, last = start * each, (start + len(outs)) * each
    beyond = far[total + first : total + last, :]
    wide = weights.shape[1]
    for column in range(0, rows.shape[1], wide):
        row = far_first + keep.shape[0] + column // wide * depth
        product = rows[first:last, column : column + wide] + dot(
            beyond, weights[row : row + depth, :]
        )
        product = product.astype(BF16)
        for k, out in enumerate(outs):
            for j in range(wide // 128):
                to = total + (column // 128 + j) * each
                out[to : to + each, :] = product[
                    k * each : (k + 1) * each, j * 128 : (j + 1) * 128
                ]


def rim_body(x, b, c, out, done):
    first, copies = 0, []
    for k, part in enumerate((x, b, c)):
        size = part.shape[1]
        copy = pltpu.make_async_copy(
            part.at[pl.ds(part.shape[0] - RIM, RIM), :],
            out.at[:, pl.ds(first, size)],
            done.at[k],
        )
        copy.start()
        copies.append(copy)
        first += size
    for copy in copies:
        copy.wait()


def last_rows(*parts):
    width = sum(part.shape[1] for part in parts)
    return pl.pallas_call(
        rim_body,
        out_shape=shaped(RIM, width),
        in_specs=[pl.BlockSpec(memory_space=pltpu.HBM)] * len(parts),
        out_specs=VMEM,
        scratch_shapes=[pltpu.SemaphoreType.DMA((len(parts),))],
    )(*parts)


def merge_body(place, stay_up, stay_down, from_left, from_right, from_across, up, down):
    far = from_across[...].astype(F32)
    core = jnp.full((1, 1), place[0])
    total = stay_up[...].astype(F32) + from_left[...].astype(F32)
    up[...] = (total + jnp.where(core == 0, far, 0.0)).astype(BF16)
    total = stay_down[...].astype(F32) + from_right[...].astype(F32)
    down[...] = (total + jnp.where(core == 1, far, 0.0)).astype(BF16)


def total_body(stay, left, right, up, down, out, rows_out):
    total = stay[...].astype(F32) + left[...].astype(F32) + right[...].astype(F32)
    total = (total + up[...].astype(F32) + down[...].astype(F32)).astype(BF16)
    count, lanes = out.shape
    rows, width = rows_out.shape
    out[...] = total[0:count]
    for j in range(width // lanes):
        first = count + j * rows
        rows_out[:, j * lanes : (j + 1) * lanes] = total[first : first + rows]


def combine_body(got, slots, coefs, out):
    sources, capacity, lanes = got.shape
    rows = got[...].reshape(sources * capacity, lanes)
    slot_ids = iota((rows.shape[0], slots.shape[1]), 0)
    padded = jnp.concatenate([coefs[...]] * (8 // TOPK), axis=0)
    columns = padded.T
    total = None
    for k in range(TOPK):
        chosen = (slot_ids == slots[k : k + 1, :]).astype(F32).astype(BF16)
        term = dot(chosen, rows, (0, 0)) * columns[:, k : k + 1]
        total = term if total is None else total + term
    out[...] = total.astype(BF16)


def local(
    blender_incoming_features,
    entry_latent_matrix,
    exit_latent_matrix,
    unactivated_valve,
    presoftplus_strides,
    extra_attenuation,
    incoming_feature_kernel,
    entry_latent_kernel,
    exit_latent_kernel,
    stride_offset_vector,
    attenuation_speed_exponent,
    bypass_coef_vector,
    cluster_rescale_coefs,
    blender_result_matrix,
    latter_microbatch_activations,
    specialist_rescale_coefs,
    specialist_valve_matrix,
    specialist_expand_matrix,
    specialist_contract_matrix,
    specialist_picks,
    selected_specialist_coefs,
):
    ep_count, chips = lax.axis_size(EP), lax.axis_size("tp_0")
    chip, core = lax.axis_index("tp_0"), lax.axis_index("tp_1")
    count, width = blender_incoming_features.shape
    state = entry_latent_matrix.shape[1]
    token_count, model_width = latter_microbatch_activations.shape
    capacity = 3 * token_count * TOPK // (2 * ep_count)
    lanes = model_width // lax.axis_size(TP)
    total_rows = ep_count * capacity
    place = (core.reshape(1), chip.reshape(1))
    valve = specialist_valve_matrix.reshape(model_width, -1)
    expand = specialist_expand_matrix.reshape(model_width, -1)
    contract = specialist_contract_matrix.reshape(-1, model_width)
    hidden_width = valve.shape[1]

    def permuted(x, axis, pairs):
        return lax.ppermute(x, axis, pairs)

    def around(x, distance):
        return permuted(x, "tp_0", [(i, (i + distance) % chips) for i in range(chips)])

    def across(x):
        pairs = []
        for i in range(chips):
            pairs.append((2 * i, 2 * ((i + 2) % chips)))
            pairs.append((2 * i + 1, 2 * ((i - 2) % chips) + 1))
        return permuted(x, TP, pairs)

    def partner(x):
        return permuted(x, "tp_1", [(0, 1), (1, 0)])

    def exchanged(x, axis):
        return lax.all_to_all(x, axis, 0, 0, tiled=True)

    rim = last_rows(blender_incoming_features, entry_latent_matrix, exit_latent_matrix)
    rim = permuted(rim, EP, [(i, i + 1) for i in range(ep_count - 1)])
    taps = (incoming_feature_kernel, entry_latent_kernel, exit_latent_kernel)
    filtered_shapes = (
        shaped(count, width, dtype=F32),
        shaped(count, state),
        shaped(count, state),
    )
    routed, slots, x, b, c, heads, columns, rows = call(
        functools.partial(route_body, ep_count),
        (
            shaped(total_rows, 2 * lanes),
            shaped(TOPK, token_count, dtype=jnp.int32),
            *filtered_shapes,
            shaped(RIM, width + 2 * state, dtype=F32),
            shaped(count, 8, dtype=F32),
            shaped(8, count, dtype=F32),
        ),
        (
            (core * (chips // 2) + chip % (chips // 2)).reshape(1),
            stride_offset_vector,
            attenuation_speed_exponent,
            latter_microbatch_activations,
            specialist_rescale_coefs,
            specialist_picks.T,
            blender_incoming_features,
            entry_latent_matrix,
            exit_latent_matrix,
            *taps,
            presoftplus_strides.T,
            extra_attenuation.T,
        ),
        1 << 30,
        None,
        scratch=(pltpu.VMEM((RIM + count, width + 2 * state), F32),),
        smem=3,
    )
    send, x, b, c = call(
        filter_body,
        (shaped(ep_count, 2 * capacity + 2 * PIECE, lanes), *filtered_shapes),
        (routed, x, b, c, heads, rim, *taps, columns),
        1 << 30,
        None,
        scratch=(pltpu.VMEM((2 * RIM, width + 2 * state), F32),),
    )
    got = exchanged(send, EP)
    y = inside(bypass_coef_vector, x, b, c, columns, rows)

    half = model_width // 2
    keep, give = call(
        placed(split_body),
        (shaped(half, hidden_width), shaped(5 * half, hidden_width)),
        (*place, valve, expand, contract, blender_result_matrix),
        1 << 30,
        None,
        smem=2,
    )
    weights_far = partner(give)

    own = got[:, 0 : 2 * capacity, :]
    beyond = across(own)
    left, right = around(own, 1), around(own, -1)
    pieces = (own, left, right, beyond)
    theirs = call(
        placed(theirs_body),
        shaped(total_rows, 2 * hidden_width),
        (*place, *pieces, weights_far),
        1 << 31,
        10,
        smem=2,
    )
    theirs = partner(theirs)

    enter = call(enter_body, shaped(ep_count, PIECE, lanes), (got,), 1 << 30, 8)
    enter = exchanged(enter, EP).reshape(width, state)
    row_count = count // 2
    mine_rows, other_rows = call(
        placed(finish_body),
        (shaped(row_count, width),) * 2,
        (
            *place,
            y,
            c,
            columns,
            enter,
            unactivated_valve,
            cluster_rescale_coefs.astype(F32).reshape(-1, 128),
        ),
        1 << 31,
        8,
        scratch=(pltpu.VMEM((count, width), F32),),
        smem=2,
    )
    ours = call(
        placed(ours_body),
        shaped(total_rows + row_count, hidden_width),
        (*place, *pieces, valve, expand, theirs, other_rows),
        1 << 31,
        10,
        smem=2,
    )
    ours_far = partner(ours)
    row_block = count * model_width // (2 * chips * lanes)
    all_rows = total_rows + row_block
    projected = call(
        project_body,
        shaped(row_count, model_width, dtype=F32),
        (mine_rows, blender_result_matrix),
        1 << 29,
        6,
    )

    def partials(start):
        return call(
            functools.partial(down_body, start),
            (shaped(all_rows, lanes),) * 4,
            (ours, ours_far, projected, keep, weights_far),
            1 << 31,
            12,
        )

    for_three, for_five, for_four, for_six = partials(0)
    from_across = across(for_four)
    from_left = around(for_three, 1)
    from_right = around(for_five, -1)
    for_one, for_seven, stay, for_two = partials(4)
    left_of_me, right_of_me = around(for_one, 1), around(for_seven, -1)
    up_two, down_two = call(
        placed(merge_body),
        (shaped(all_rows, lanes),) * 2,
        (*place, for_two, for_six, from_left, from_right, from_across),
        1 << 29,
        6,
        smem=2,
    )
    from_up, from_down = around(up_two, 2), around(down_two, -2)
    summed, mixed_a = call(
        total_body,
        (shaped(total_rows, lanes), shaped(count // (2 * chips), model_width)),
        (stay, left_of_me, right_of_me, from_up, from_down),
        1 << 29,
        4,
    )
    returned = exchanged(summed.reshape(ep_count, capacity, lanes), EP)
    mixed_b = call(
        combine_body,
        shaped(token_count, lanes),
        (returned, slots, selected_specialist_coefs.T),
        1 << 28,
        8,
    )
    return (mixed_a, mixed_b)


def inside(bypass, x, b, c, columns, rows):
    def body(bypass, x, b, c, columns, rows, out):
        inside_body(x, b, c, columns, rows, bypass, out)

    return call(
        body,
        shaped(*x.shape, dtype=F32),
        (bypass, x, b, c, columns, rows),
        1 << 31,
        None,
        smem=1,
    )


def solution(mesh):
    split = Mesh(mesh.devices.reshape(8, 4, 8, 2), ("ep_0", "ep_1", "tp_0", "tp_1"))
    in_specs = (
        P(EP, TP),
        P(EP, TP),
        P(EP, TP),
        P(EP, TP),
        P(EP, TP),
        P(EP, TP),
        P(None, TP),
        P(None, TP),
        P(None, TP),
        P(TP),
        P(TP),
        P(TP),
        P(TP),
        P(TP, None),
        P(EP, None),
        P(),
        P(EP, None, TP),
        P(EP, None, TP),
        P(EP, TP, None),
        P(EP, None),
        P(EP, None),
    )
    out_specs = (P(EP_TP, None), P(EP, TP))

    return jax.shard_map(local, mesh=split, in_specs=in_specs, out_specs=out_specs, check_vma=False)
```
